512 devices in a mesh: sp: 32 (over z, x), tp: 16 (over y, core).
Axes of the slice: x: 4, y: 8, z: 8, core: 2. Of those that a mesh axis runs over, the one named last changes fastest.
Arguments:
- layer_input: bfloat16 [32, 6144, 2048], P('sp', 'tp'), may hold values from -6 to 6
- input_gain: float32 [2048], replicated, may hold values from 0.1 to 1.9
- key_weight: bfloat16 [2048, 512], P('sp', 'tp'), may hold values from -0.125 to 0.125
- value_weight: bfloat16 [2048, 512], P('sp', 'tp'), may hold values from -0.125 to 0.125
- key_gain: float32 [128], replicated, may hold values from 0.1 to 1.9
- stop_shift: bfloat16 [32, 4, 6144], P('sp', None, 'tp'), may hold values from -20 to 0
- new_query: bfloat16 [32, 16, 128], P('sp', 'tp'), may hold values from -6 to 6
- query_gain: float32 [128], replicated, may hold values from 0.1 to 1.9
- out_gain: float32 [128], replicated, may hold values from 0.1 to 1.9
Outputs:
- key_cache: bfloat16 [32, 16, 6144, 128], P('sp', 'tp')
- value_cache: bfloat16 [32, 16, 6144, 128], P('sp', 'tp')
- shift_cache: bfloat16 [32, 16, 6144], P('sp', 'tp')
- first_read: bfloat16 [32, 16, 128], P('sp', 'tp')
The draws below stay inside these ranges and needn't reach their ends.
All inputs are finite; a program needn't handle non-finite values.
Results may differ from the reference program's by a relative error of at most 0.013.
Values may be sent and summed in bfloat16 or wider, within the bound.
No kernel may reach another device: no remote copies, remote signals or barrier semaphores. Data moves between devices by JAX's collectives and lax.ppermute only.
A program may use at most 64 MiB of HBM per device.

```python
import math
import jax
import jax.numpy as jnp
from jax import lax

D = 2048
HQ = 16
KVH = 4
HEAD = 128
TOK_DEV = 384
PROMPT_LENGTH = 6144
SEQS = 32
COPIES = 4


def draw_stop_shift(key, part):
    order_key, slow_key, fast_key, block_key, cell_key, place_key, level_key = jax.random.split(key, 7)
    head_order = jax.random.permutation(order_key, KVH)
    slow_heads = (head_order < KVH // 2)[None, :, None]
    slow_rate = jax.random.uniform(slow_key, (SEQS, KVH, 1), jnp.float32, math.log(0.1 / PROMPT_LENGTH), math.log(1.0 / PROMPT_LENGTH))
    fast_rate = jax.random.uniform(fast_key, (SEQS, KVH, 1), jnp.float32, math.log(4.0 / TOK_DEV), math.log(12.0 / TOK_DEV))
    log_rate = jnp.where(slow_heads, slow_rate, fast_rate)
    blocks = jax.random.uniform(block_key, (SEQS, KVH, PROMPT_LENGTH // TOK_DEV, 1), jnp.float32, -0.7, 0.7)
    blocks = jnp.broadcast_to(blocks, (SEQS, KVH, PROMPT_LENGTH // TOK_DEV, TOK_DEV)).reshape(SEQS, KVH, PROMPT_LENGTH)
    cell_noise = jax.random.uniform(cell_key, (SEQS, KVH, PROMPT_LENGTH), jnp.float32, -0.7, 0.7)
    baseline_offset = jnp.minimum(log_rate + blocks + cell_noise, -0.5)
    token_positions = jax.random.randint(place_key, (SEQS, 1, 1, 4), 0, PROMPT_LENGTH)
    spike_mask = jnp.any(jnp.arange(PROMPT_LENGTH)[None, None, :, None] == token_positions, axis=-1)
    depth_levels = jax.random.uniform(level_key, (SEQS, KVH, PROMPT_LENGTH), jnp.float32, -1.4, 0.0)
    return jnp.where(spike_mask, depth_levels, baseline_offset).astype(jnp.bfloat16)


def levels(rng, dims, cuts, low, top_value):
    def one(axis_at, blocks):
        draws = jax.random.uniform(jax.random.fold_in(jax.random.fold_in(rng, 6), axis_at), (blocks,), jnp.float32, low / len(cuts), top_value / len(cuts))
        return jnp.repeat(jnp.exp(draws), dims[axis_at] // blocks).reshape((-1,) + (1,) * (len(dims) - axis_at - 1))

    level = one(*cuts[0])
    for cut in cuts[1:]:
        level = level * one(*cut)
    return level


def normal_values(rng, shape, spread, limit, cuts=(), dtype=jnp.bfloat16):
    entries = jax.random.normal(rng, shape, jnp.float32) * spread
    if len(cuts) > 0:
        entries = levels(rng, shape, cuts, -0.22, 0.18) * entries
    return jnp.clip(entries, min=-limit, max=limit).astype(dtype)


def setup_inputs(seed: int = 0) -> dict:
    key_of = jax.random.split(jax.random.key(seed), 10)
    layer_input = normal_values(key_of[0], (SEQS, PROMPT_LENGTH, D), 1.0, 6.0, ((0, 32), (1, 16)))
    input_gain = jnp.clip(1.0 + 0.18 * jax.random.normal(key_of[1], (D,), jnp.float32), 0.1, 1.9)
    key_weight = normal_values(key_of[2], (D, KVH * HEAD), D ** -0.5, 0.125, ((0, 32), (1, 16)))
    value_weight = normal_values(key_of[3], (D, KVH * HEAD), D ** -0.5, 0.125, ((0, 32), (1, 16)))
    key_gain = jnp.clip(1.0 + 0.18 * jax.random.normal(key_of[4], (HEAD,), jnp.float32), 0.1, 1.9)
    stop_shift = draw_stop_shift(jax.random.fold_in(key_of[9], 71), 0)
    new_query = normal_values(key_of[6], (SEQS, HQ, HEAD), 1.0, 6.0, ((0, 32), (1, 16)))
    query_gain = jnp.clip(1.0 + 0.18 * jax.random.normal(key_of[7], (HEAD,), jnp.float32), 0.1, 1.9)
    out_gain = jnp.clip(1.0 + 0.18 * jax.random.normal(key_of[8], (HEAD,), jnp.float32), 0.1, 1.9)
    return dict(layer_input=layer_input, input_gain=input_gain, key_weight=key_weight, value_weight=value_weight, key_gain=key_gain, stop_shift=stop_shift, new_query=new_query, query_gain=query_gain, out_gain=out_gain)


epsilon = 1e-06

def row_norm(value_entries, scaling):
    return value_entries * lax.rsqrt(lax.optimization_barrier(jnp.mean(value_entries * value_entries, axis=-1, keepdims=True)) + epsilon) * scaling

def reference(layer_input, input_gain, key_weight, value_weight, key_gain, stop_shift, new_query, query_gain, out_gain):
    group_size = HQ // KVH
    score_scale = 1.0 / HEAD ** 0.5

    def one_sequence(sequence):
        tokens, shifts, queries = sequence
        normed = row_norm(tokens.astype(jnp.float32), input_gain).astype(jnp.bfloat16)
        raw_keys = jnp.dot(normed, key_weight, preferred_element_type=jnp.float32).reshape(PROMPT_LENGTH, KVH, HEAD)
        key_rows = row_norm(raw_keys, key_gain).astype(jnp.bfloat16)
        value_rows = jnp.dot(normed, value_weight, preferred_element_type=jnp.float32).astype(jnp.bfloat16).reshape(PROMPT_LENGTH, KVH, HEAD)
        query_rows = row_norm(queries.astype(jnp.float32), query_gain).astype(jnp.bfloat16).reshape(KVH, group_size, HEAD)
        scores = jnp.einsum('kgd,lkd->kgl', query_rows.astype(jnp.float32), key_rows.astype(jnp.float32)) * score_scale
        scores = scores + shifts.astype(jnp.float32)[:, None, :]
        log_keep = jax.nn.log_sigmoid(-scores)
        later_sum = lax.cumsum(log_keep, axis=2, reverse=True) - log_keep
        weights = jnp.exp(jax.nn.log_sigmoid(scores) + later_sum).astype(jnp.bfloat16)
        read_sum = jnp.einsum('kgl,lkd->kgd', weights.astype(jnp.float32), value_rows.astype(jnp.float32)).reshape(HQ, HEAD)
        first_out = row_norm(read_sum, out_gain).astype(jnp.bfloat16)
        key_slots = jnp.repeat(key_rows.transpose(1, 0, 2), COPIES, axis=0)
        value_slots = jnp.repeat(value_rows.transpose(1, 0, 2), COPIES, axis=0)
        shift_slots = jnp.repeat(shifts, COPIES, axis=0)
        return (key_slots, value_slots, shift_slots, first_out)
    key_cache, value_cache, shift_cache, first_read = lax.map(one_sequence, (layer_input, stop_shift, new_query))
    return (key_cache, value_cache, shift_cache, first_read)
```

```python
import jax
import jax.numpy as jnp
from jax import lax
from jax.experimental import pallas as pl
from jax.experimental.pallas import tpu as pltpu
from jax.sharding import PartitionSpec as P

KVH = 4
NX = 4
epsilon = 1e-06


def row_norm(value_entries, scaling):
    return (
        value_entries
        * lax.rsqrt(jnp.mean(value_entries * value_entries, axis=-1, keepdims=True) + epsilon)
        * scaling
    )


def moved_sp(x, dz, dx):
    n = lax.axis_size("sp")
    nz = n // NX
    pairs = []
    for i in range(n):
        z, c = (i // NX + dz) % nz, (i % NX + dx) % NX
        pairs.append((i, z * NX + c))
    return lax.ppermute(x, "sp", pairs)


def moved_y(x, target):
    n = lax.axis_size("tp")
    return lax.ppermute(x, "tp", [(i, target(i // 2) % (n // 2) * 2 + i % 2) for i in range(n)])


def swapped(x):
    return lax.ppermute(x, "tp", [(i, i ^ 1) for i in range(lax.axis_size("tp"))])


def step_to(distance):
    sign = -1 if distance % 2 else 1
    return lambda y: y + sign * distance if y % 2 == 0 else y - sign * distance


def packed(w):
    rows, cols = w.shape
    n = 128 // cols
    return w.reshape(n, rows // n, cols).transpose(1, 0, 2).reshape(rows // n, 128)


def build_body(recv, whole, low, high, *, blocks):
    lane = lax.broadcasted_iota(jnp.int32, (16 * blocks, 128), 1) // 32
    half = blocks // 2
    for head in range(KVH):
        parts = [recv[4 * head + t, : 16 * blocks, :].astype(jnp.float32) for t in range(4)]
        for q in range(4):
            out = None
            for t in range(4):
                shift = 32 * ((t - q) % 4)
                turned = pltpu.roll(parts[t], shift, 1) if shift else parts[t]
                out = turned if out is None else jnp.where(lane == t, turned, out)
            out = out.astype(jnp.bfloat16).reshape(blocks, 16, 128)
            cols = slice(128 * head, 128 * head + 128)
            whole[:, q, :, cols] = out
            low[:, q, :, cols] = out[:half]
            high[:, q, :, cols] = out[half:]


def project_body(meta, own, other, w0, wl, wr, wu, wd, gain, *rest):
    outs, wide, line = rest[:4], rest[4], rest[5]
    cls, core = meta[0], meta[1]

    def put(ref, c, at, first, count):
        for b in range(count):
            x = lax.rem(c + 2 * ((first + b) % 2), NX)
            to = pl.multiple_of(256 * (first + b) + 64 * x, 64)
            wide[pl.ds(to, 64), :] = ref[64 * (at + b) : 64 * (at + b) + 64, :]

    put(w0, cls, 0, 0, 8)
    put(wl, lax.rem(cls + 3, NX), 0, 0, 8)
    put(wr, lax.rem(cls + 1, NX), 0, 0, 8)
    put(wu, lax.rem(cls + 2, NX), 0, 0, 4)
    put(wd, lax.rem(cls + 2, NX), 0, 4, 4)
    rows = own.shape[0]
    is_key = core == 0
    for ref, place in ((own, core), (other, 1 - core)):
        acc = jnp.dot(ref[...], wide[...], preferred_element_type=jnp.float32)
        to = pl.multiple_of(place * rows, 128)
        for head in range(KVH):
            a = acc[:, 128 * head : 128 * head + 128]
            normed = row_norm(a, gain[...])
            line[pl.ds(to, rows), 128 * head : 128 * head + 128] = jnp.where(
                is_key, normed, a
            ).astype(jnp.bfloat16)
    for slot in range(4):
        at = pl.multiple_of(128 * meta[2 + slot], 128)
        outs[slot][...] = line[:, pl.ds(at, 128)]


def read_body(meta, query, query_gain, out_gain, shift, *rest, size, blocks, scale):
    mine, theirs = rest[:8], rest[8:11]
    keys, values, first = rest[11:14]
    score_ref, weight_ref, sems = rest[14:]
    theirs_of = [
        (0, 0),
        (0, 1),
        (0, 2),
        (1, 0),
        (1, 3),
        (1, 1),
        (1, 2),
        (2, 0),
    ]
    per = size // 128

    def their(j):
        part, at = theirs_of[j]
        return theirs[part].at[pl.ds(at * size, size), :]

    q = row_norm(query[...].astype(jnp.float32), query_gain[...]).astype(jnp.bfloat16)
    q = jnp.broadcast_to(q, (16, 128))

    def run(key_of, value_of):
        copies = []
        for j in range(8):
            at = pl.multiple_of(meta[2 + j] * size, 128)
            copies.append(
                pltpu.make_async_copy(key_of(j), keys.at[pl.ds(at, size), :], sems.at[j])
            )
            copies.append(
                pltpu.make_async_copy(value_of(j), values.at[pl.ds(at, size), :], sems.at[8 + j])
            )
        for c in copies:
            c.start()
        for j in range(8):
            s = lax.dot_general(
                q, key_of(j)[...], (((1,), (1,)), ((), ())), preferred_element_type=jnp.float32
            )
            for i in range(per):
                score_ref[pl.ds(meta[2 + j] * per + i, 1), :] = s[0:1, 128 * i : 128 * i + 128]
        s = score_ref[...] * scale + shift[...].astype(jnp.float32)
        keep = jax.nn.log_sigmoid(-s)
        lower = lax.broadcasted_iota(jnp.int32, (128, 128), 0)
        tri = (lower > lax.broadcasted_iota(jnp.int32, (128, 128), 1)).astype(jnp.float32)
        inside = jnp.dot(
            keep, tri, precision=lax.Precision.HIGHEST, preferred_element_type=jnp.float32
        )
        row = lax.broadcasted_iota(jnp.int32, (blocks, blocks), 0)
        up = (lax.broadcasted_iota(jnp.int32, (blocks, blocks), 1) > row).astype(jnp.float32)
        later = jnp.dot(
            up, keep, precision=lax.Precision.HIGHEST, preferred_element_type=jnp.float32
        )
        inside = inside + jnp.sum(later, axis=1, keepdims=True)
        weight_ref[...] = jnp.exp(jax.nn.log_sigmoid(s) + inside)
        total = jnp.zeros((16, 128), jnp.float32)
        for j in range(8):
            ref = value_of(j)
            for i in range(per):
                w = weight_ref[pl.ds(meta[2 + j] * per + i, 1), :].astype(jnp.bfloat16)
                total = total + jnp.dot(
                    jnp.broadcast_to(w, (16, 128)),
                    ref[128 * i : 128 * i + 128, :],
                    preferred_element_type=jnp.float32,
                )
        first[...] = row_norm(total[0:1], out_gain[...]).astype(jnp.bfloat16)
        for c in copies:
            c.wait()

    @pl.when(meta[1] == 0)
    def _():
        run(lambda j: mine[j], their)

    @pl.when(meta[1] == 1)
    def _():
        run(their, lambda j: mine[j])


def in_vmem(n):
    return [pl.BlockSpec(memory_space=pltpu.VMEM)] * n


def in_smem():
    return [pl.BlockSpec(memory_space=pltpu.SMEM)]


def shards(
    layer_input,
    input_gain,
    key_weight,
    value_weight,
    key_gain,
    stop_shift,
    new_query,
    query_gain,
    out_gain,
):
    groups = lax.axis_size("tp")
    n_sp = lax.axis_size("sp")
    nz, ny = n_sp // NX, groups // 2
    rows = layer_input.shape[1]
    size = 2 * rows
    head_size = new_query.shape[2]
    length = rows * groups
    place = lax.axis_index("tp")
    y, core = place // 2, place % 2
    at_sp = lax.axis_index("sp")
    cls = (at_sp % NX + 2 * (at_sp // NX)) % NX

    own = jnp.concatenate((packed(key_weight), packed(value_weight)), 0)
    classes = [[z * NX + (c + 2 * z) % NX for z in range(nz)] for c in range(NX)]
    got = lax.all_to_all(
        jnp.broadcast_to(own, (nz, *own.shape)),
        "sp",
        split_axis=0,
        concat_axis=0,
        tiled=True,
        axis_index_groups=classes,
    )
    deep = 16 * nz
    both = got.reshape(nz, 2, 16, 128).transpose(1, 0, 2, 3).reshape(2, deep, 128)
    shifts = jnp.pad(stop_shift[0].reshape(KVH, rows // 128, 128), ((0, 0), (0, 13), (0, 0)))
    sent = jnp.concatenate(
        (
            jnp.broadcast_to(both[None], (ny, 2, deep, 128)).reshape(groups, deep, 128),
            jnp.repeat(shifts, groups // KVH, axis=0),
        ),
        axis=1,
    )
    recv = lax.all_to_all(sent, "tp", split_axis=0, concat_axis=0, tiled=True)
    shift_line = recv[:, deep : deep + rows // 128, :].reshape(length // 128, 128)
    cols = KVH * head_size
    w0, low, high = pl.pallas_call(
        lambda *refs: build_body(*refs, blocks=nz),
        out_shape=(
            jax.ShapeDtypeStruct((nz, 4, 16, cols), jnp.bfloat16),
            jax.ShapeDtypeStruct((nz // 2, 4, 16, cols), jnp.bfloat16),
            jax.ShapeDtypeStruct((nz // 2, 4, 16, cols), jnp.bfloat16),
        ),
        in_specs=in_vmem(1),
        out_specs=tuple(in_vmem(3)),
        name="build",
    )(recv)
    w0 = w0.reshape(nz * 64, cols)
    low, high = low.reshape(nz * 32, cols), high.reshape(nz * 32, cols)
    wl = moved_sp(w0, 0, 1)
    wr = moved_sp(w0, 0, -1)
    wu = moved_sp(low, 1, 0)
    wd = moved_sp(high, -1, 0)

    normed = row_norm(layer_input[0].astype(jnp.float32), input_gain).astype(jnp.bfloat16)
    other = swapped(normed)

    pair = y // 2
    sign = jnp.where(y % 2 == 0, -1, 1)
    heads = [pair, pair + sign, pair - sign, pair + 2]
    meta = jnp.stack([cls, core] + [(h + KVH) % KVH for h in heads]).astype(jnp.int32)
    slots = pl.pallas_call(
        project_body,
        out_shape=tuple(jax.ShapeDtypeStruct((size, head_size), jnp.bfloat16) for _ in range(4)),
        in_specs=in_smem() + in_vmem(8),
        out_specs=tuple(in_vmem(4)),
        scratch_shapes=[
            pltpu.VMEM((n_sp * 64, cols), jnp.bfloat16),
            pltpu.VMEM((size, cols), jnp.bfloat16),
        ],
        name="project",
    )(meta, normed, other, w0, wl, wr, wu, wd, key_gain.reshape(1, head_size))

    across = lambda at: at ^ 1
    mine0 = slots[0]
    p1 = moved_y(slots[1], step_to(1))
    p2 = moved_y(slots[2], step_to(2))
    p3 = moved_y(slots[3], step_to(3))
    f0 = moved_y(mine0, across)
    f1 = moved_y(p1, across)
    f2 = moved_y(p2, across)
    f3 = moved_y(p3, across)
    t1 = swapped(jnp.concatenate((mine0, f0, p1), 0))
    t2 = swapped(jnp.concatenate((p2, f1, f2, p3), 0))
    t3 = swapped(f3)
    beside = y + 1 - 2 * (y % 2)
    sources = [y, beside] + [y + sign * d for d in (1, 2, 3)] + [beside - sign * d for d in (1, 2, 3)]
    meta2 = jnp.stack([y, core] + [(s + ny) % ny for s in sources]).astype(jnp.int32)
    key_line, value_line, first_out = pl.pallas_call(
        lambda *refs: read_body(
            *refs, size=size, blocks=length // 128, scale=1.0 / head_size**0.5
        ),
        out_shape=(
            jax.ShapeDtypeStruct((length, head_size), jnp.bfloat16),
            jax.ShapeDtypeStruct((length, head_size), jnp.bfloat16),
            jax.ShapeDtypeStruct((1, head_size), jnp.bfloat16),
        ),
        in_specs=in_smem() + in_vmem(15),
        out_specs=(
            pl.BlockSpec(memory_space=pl.ANY),
            pl.BlockSpec(memory_space=pl.ANY),
            pl.BlockSpec(memory_space=pltpu.VMEM),
        ),
        scratch_shapes=[
            pltpu.VMEM((length // 128, 128), jnp.float32),
            pltpu.VMEM((length // 128, 128), jnp.float32),
            pltpu.SemaphoreType.DMA((16,)),
        ],
        name="read",
    )(
        meta2,
        new_query[0],
        query_gain.reshape(1, head_size),
        out_gain.reshape(1, head_size),
        shift_line,
        mine0,
        f0,
        p1,
        p2,
        p3,
        f1,
        f2,
        f3,
        t1,
        t2,
        t3,
    )
    return (
        key_line.reshape(1, 1, length, head_size),
        value_line.reshape(1, 1, length, head_size),
        shift_line.reshape(1, 1, length),
        first_out[None],
    )


def solution(mesh):
    placed = (
        P("sp", "tp", None),
        P(),
        P("sp", "tp"),
        P("sp", "tp"),
        P(),
        P("sp", None, "tp"),
        P("sp", "tp", None),
        P(),
        P(),
    )
    return jax.shard_map(
        shards,
        mesh=mesh,
        in_specs=placed,
        out_specs=(
            P("sp", "tp", None, None),
            P("sp", "tp", None, None),
            P("sp", "tp", None),
            P("sp", "tp", None),
        ),
        check_vma=False,
    )
```

```python
import jax
import jax.numpy as jnp
from jax import lax
from jax.experimental import pallas as pl
from jax.experimental.pallas import tpu as pltpu
from jax.sharding import PartitionSpec as P

KVH = 4
NX = 4
CLASSES = 4
epsilon = 1e-06


def row_norm(value_entries, scaling):
    return (
        value_entries
        * lax.rsqrt(jnp.mean(value_entries * value_entries, axis=-1, keepdims=True) + epsilon)
        * scaling
    )


def moved_sp(x, dz, dx):
    n = lax.axis_size("sp")
    nz = n // NX
    pairs = []
    for i in range(n):
        z, c = (i // NX + dz) % nz, (i % NX + dx) % NX
        pairs.append((i, z * NX + c))
    return lax.ppermute(x, "sp", pairs)


def moved_y(x, target):
    n = lax.axis_size("tp")
    return lax.ppermute(
        x, "tp", [(i, target(i // 2) % (n // 2) * 2 + i % 2) for i in range(n)]
    )


def swapped(x):
    return lax.ppermute(x, "tp", [(i, i ^ 1) for i in range(lax.axis_size("tp"))])


def step_to(distance):
    sign = -1 if distance % 2 else 1
    return lambda y: y + sign * distance if y % 2 == 0 else y - sign * distance


def chip_and_core():
    place = lax.axis_index("tp")
    return lax.div(place, 2), lax.rem(place, 2)


def own_class():
    at = lax.axis_index("sp")
    return lax.rem(lax.rem(at, NX) + 2 * lax.div(at, NX), CLASSES)


def pack_body(key_t, value_t, shift, out):
    groups = out.shape[0]
    zeros = jnp.zeros((13, 128), jnp.float32)
    rows = []
    for ref in (key_t, value_t):
        w = ref[...].astype(jnp.float32)
        rows.append(jnp.concatenate((w[:16], w[16:]), axis=1).astype(jnp.bfloat16))
    lines = shift[...].astype(jnp.float32)
    for head in range(KVH):
        parts = [lines[head : head + 1, 128 * i : 128 * i + 128] for i in range(3)]
        tail = jnp.concatenate((*parts, zeros), axis=0).astype(jnp.bfloat16)
        for i in range(groups // KVH):
            peer = head * (groups // KVH) + i
            out[peer, :16, :] = rows[peer % 2]
            out[peer, 16:, :] = tail


def build_body(recv, blocks, shift48, shift_line, tall, lines):
    groups = recv.shape[0]
    for t in range(groups):
        a = recv[t, :16, :].astype(jnp.float32)
        tall[32 * t : 32 * t + 16, :] = a[:, :64].astype(jnp.bfloat16)
        tall[32 * t + 16 : 32 * t + 32, :] = a[:, 64:].astype(jnp.bfloat16)
        tail = recv[t, 16:, :].astype(jnp.float32)
        lines[3 * t : 3 * t + 3, :] = tail[:3]
    i = lax.broadcasted_iota(jnp.int32, (64, 64), 0)
    eye = (i == lax.broadcasted_iota(jnp.int32, (64, 64), 1)).astype(jnp.bfloat16)
    wide = lax.dot_general(
        eye, tall[...], (((1,), (1,)), ((), ())), preferred_element_type=jnp.float32
    ).astype(jnp.bfloat16)
    for b in range(blocks.shape[0]):
        blocks[b] = wide
    shift48[...] = lines[...]
    for r in range(3 * groups):
        shift_line[0, :, 128 * r : 128 * r + 128] = lines[r : r + 1, :].astype(jnp.bfloat16)


def norm_body(x, gain, out):
    n = row_norm(x[...].astype(jnp.float32), gain[...])
    width = out.shape[1] // CLASSES
    for c in range(CLASSES):
        for m in range(width // 128):
            a = 512 * m + 64 * c
            b = 512 * m + 256 + 64 * ((c + 2) % CLASSES)
            both = jnp.concatenate((n[:, a : a + 64], n[:, b : b + 64]), axis=1)
            out[:, width * c + 128 * m : width * c + 128 * m + 128] = both.astype(jnp.bfloat16)


def columns(ref, c, at, count):
    width = ref.shape[1] // CLASSES
    return ref[:, pl.ds(pl.multiple_of(c * width + at, 128), count)]


def first_body(own, other, w0, acc):
    c = own_class()
    for i, ref in enumerate((own, other)):
        x = columns(ref, c, 0, w0.shape[0])
        acc[i] = jnp.dot(x, w0[...], preferred_element_type=jnp.float32)


def sides_body(own, other, wl, wr, acc, out):
    c = own_class()
    for i, ref in enumerate((own, other)):
        total = acc[i]
        for w, step in ((wl, 3), (wr, 1)):
            x = columns(ref, lax.rem(c + step, CLASSES), 0, w.shape[0])
            total = total + jnp.dot(x, w[...], preferred_element_type=jnp.float32)
        out[i] = total


def last_body(own, other, wu, wd, acc, gain, *rest):
    outs, line = rest[:4], rest[4]
    c = lax.rem(own_class() + 2, CLASSES)
    y, core = chip_and_core()
    rows, half = own.shape[0], wu.shape[0]
    is_key = core == 0
    for i, ref in enumerate((own, other)):
        total = acc[i]
        for w, at in ((wu, 0), (wd, half)):
            x = columns(ref, c, at, half)
            total = total + jnp.dot(x, w[...], preferred_element_type=jnp.float32)
        to = pl.multiple_of((core if i == 0 else 1 - core) * rows, 128)
        for head in range(KVH):
            a = total[:, 128 * head : 128 * head + 128]
            line[pl.ds(to, rows), 128 * head : 128 * head + 128] = jnp.where(
                is_key, row_norm(a, gain[...]), a
            ).astype(jnp.bfloat16)
    pair = lax.div(y, 2)
    sign = 2 * lax.rem(y, 2) - 1
    for slot, head in enumerate((pair, pair + sign, pair - sign, pair + 2)):
        at = pl.multiple_of(128 * lax.rem(head + KVH, KVH), 128)
        outs[slot][...] = line[:, pl.ds(at, 128)]


def read_body(query, query_gain, out_gain, shift, *rest, size, scale, chips):
    mine, theirs = rest[:8], rest[8:11]
    keys, values, first = rest[11:14]
    score_ref, weight_ref, sems = rest[14:]
    theirs_of = [(0, 0), (0, 1), (0, 2), (1, 0), (1, 3), (1, 1), (1, 2), (2, 0)]
    per = size // 128
    blocks = chips * per
    y, core = chip_and_core()
    sign = 2 * lax.rem(y, 2) - 1
    beside = y - sign
    sources = [y, beside] + [y + sign * d for d in (1, 2, 3)] + [beside - sign * d for d in (1, 2, 3)]
    sources = [lax.rem(s + chips, chips) for s in sources]

    def their(j):
        part, at = theirs_of[j]
        return theirs[part].at[pl.ds(at * size, size), :]

    q = row_norm(query[...].astype(jnp.float32), query_gain[...]).astype(jnp.bfloat16)
    rows = lax.broadcasted_iota(jnp.int32, (128, 128), 0)
    lanes = lax.broadcasted_iota(jnp.int32, (128, 128), 1)
    on = rows == lanes
    q_all = jnp.broadcast_to(q, (128, 128))
    ones = jnp.ones((128, 128), jnp.bfloat16)

    def run(key_of, value_of):
        copies = []
        for j in range(8):
            at = pl.multiple_of(sources[j] * size, 128)
            copies.append(
                pltpu.make_async_copy(key_of(j), keys.at[pl.ds(at, size), :], sems.at[j])
            )
            copies.append(
                pltpu.make_async_copy(value_of(j), values.at[pl.ds(at, size), :], sems.at[8 + j])
            )
        for c in copies:
            c.start()
        for j in range(8):
            s = lax.dot_general(
                key_of(j)[...], q_all, (((1,), (1,)), ((), ())), preferred_element_type=jnp.float32
            )
            for i in range(per):
                line = jnp.sum(
                    jnp.where(on, s[128 * i : 128 * i + 128], 0.0), axis=0, keepdims=True
                )
                score_ref[pl.ds(sources[j] * per + i, 1), :] = line
        s = score_ref[...] * scale + shift[...]
        keep = jax.nn.log_sigmoid(-s)
        inside = jnp.dot(
            keep,
            (rows > lanes).astype(jnp.float32),
            precision=lax.Precision.HIGHEST,
            preferred_element_type=jnp.float32,
        )
        at_row = lax.broadcasted_iota(jnp.int32, (blocks, blocks), 0)
        up = (lax.broadcasted_iota(jnp.int32, (blocks, blocks), 1) > at_row).astype(jnp.float32)
        later = jnp.dot(
            up, keep, precision=lax.Precision.HIGHEST, preferred_element_type=jnp.float32
        )
        inside = inside + jnp.sum(later, axis=1, keepdims=True)
        weight_ref[...] = jnp.exp(jax.nn.log_sigmoid(s) + inside)
        total = jnp.zeros((128, 128), jnp.float32)
        for j in range(8):
            ref = value_of(j)
            for i in range(per):
                w = weight_ref[pl.ds(sources[j] * per + i, 1), :]
                spread = jnp.where(on, w, 0.0).astype(jnp.bfloat16)
                spread = jnp.dot(spread, ones, preferred_element_type=jnp.float32)
                total = total + spread * ref[128 * i : 128 * i + 128, :].astype(jnp.float32)
        total = jnp.sum(total, axis=0, keepdims=True)
        first[...] = row_norm(total, out_gain[...]).astype(jnp.bfloat16)
        for c in copies:
            c.wait()

    @pl.when(core == 0)
    def _():
        run(lambda j: mine[j], their)

    @pl.when(core == 1)
    def _():
        run(their, lambda j: mine[j])


def in_vmem(n):
    return [pl.BlockSpec(memory_space=pltpu.VMEM)] * n


def shape(*dims, dtype=jnp.bfloat16):
    return jax.ShapeDtypeStruct(dims, dtype)


def shards(
    layer_input,
    input_gain,
    key_weight,
    value_weight,
    key_gain,
    stop_shift,
    new_query,
    query_gain,
    out_gain,
):
    groups = lax.axis_size("tp")
    n_sp = lax.axis_size("sp")
    nz, ny = n_sp // NX, groups // 2
    rows, width = layer_input.shape[1:]
    size = 2 * rows
    head_size = new_query.shape[2]
    length = rows * groups
    cols = KVH * head_size
    deep = width // n_sp

    sent = pl.pallas_call(
        pack_body,
        out_shape=shape(groups, 32, 128),
        in_specs=in_vmem(3),
        out_specs=in_vmem(1)[0],
        name="pack",
    )(key_weight.T, value_weight.T, stop_shift[0])
    recv = lax.all_to_all(sent, "tp", split_axis=0, concat_axis=0, tiled=True)
    own = pl.pallas_call(
        norm_body,
        grid=(4,),
        out_shape=shape(rows, width),
        in_specs=[
            pl.BlockSpec((rows // 4, width), lambda i: (i, 0)),
            pl.BlockSpec((1, width), lambda i: (0, 0)),
        ],
        out_specs=pl.BlockSpec((rows // 4, width), lambda i: (i, 0)),
        name="norm",
    )(layer_input[0], input_gain.reshape(1, width))
    other = swapped(own)
    blocks, shift48, shift_line = pl.pallas_call(
        build_body,
        out_shape=(
            shape(nz, deep, cols),
            shape(length // 128, 128, dtype=jnp.float32),
            shape(1, 1, length),
        ),
        in_specs=in_vmem(1),
        out_specs=tuple(in_vmem(3)),
        scratch_shapes=[
            pltpu.VMEM((cols, deep), jnp.bfloat16),
            pltpu.VMEM((length // 128, 128), jnp.float32),
        ],
        name="build",
    )(recv)

    classes = [[z * NX + (c + 2 * z) % NX for z in range(nz)] for c in range(CLASSES)]
    got = lax.all_to_all(
        blocks, "sp", split_axis=0, concat_axis=0, tiled=True, axis_index_groups=classes
    )
    w0 = got.reshape(nz * deep, cols)
    half = nz * deep // 2
    wl = moved_sp(w0, 0, 1)
    wr = moved_sp(w0, 0, -1)
    wu = moved_sp(w0[:half], 1, 0)
    wd = moved_sp(w0[half:], -1, 0)
    acc_shape = shape(2, rows, cols, dtype=jnp.float32)
    acc = pl.pallas_call(
        first_body,
        out_shape=acc_shape,
        in_specs=in_vmem(3),
        out_specs=in_vmem(1)[0],
        cost_estimate=pl.CostEstimate(flops=4 * rows * half * cols * 2, bytes_accessed=0, transcendentals=0),
        name="first",
    )(own, other, w0)
    acc = pl.pallas_call(
        sides_body,
        out_shape=acc_shape,
        in_specs=in_vmem(5),
        out_specs=in_vmem(1)[0],
        input_output_aliases={4: 0},
        cost_estimate=pl.CostEstimate(flops=8 * rows * half * cols * 2, bytes_accessed=0, transcendentals=0),
        name="sides",
    )(own, other, wl, wr, acc)
    slots = pl.pallas_call(
        last_body,
        out_shape=tuple(shape(size, head_size) for _ in range(4)),
        in_specs=in_vmem(6),
        out_specs=tuple(in_vmem(4)),
        scratch_shapes=[pltpu.VMEM((size, cols), jnp.bfloat16)],
        cost_estimate=pl.CostEstimate(flops=4 * rows * half * cols * 2, bytes_accessed=0, transcendentals=0),
        name="last",
    )(own, other, wu, wd, acc, key_gain.reshape(1, head_size))

    def across(at):
        return at ^ 1

    mine = slots[0]
    p1 = moved_y(slots[1], step_to(1))
    p2 = moved_y(slots[2], step_to(2))
    p3 = moved_y(slots[3], step_to(3))
    f0 = moved_y(mine, across)
    f1 = moved_y(p1, across)
    f2 = moved_y(p2, across)
    f3 = moved_y(p3, across)
    t1 = swapped(jnp.concatenate((mine, f0, p1), 0))
    t2 = swapped(jnp.concatenate((p2, f1, f2, p3), 0))
    t3 = swapped(f3)
    key_line, value_line, first_out = pl.pallas_call(
        lambda *refs: read_body(*refs, size=size, scale=1.0 / head_size**0.5, chips=ny),
        out_shape=(
            shape(length, head_size),
            shape(length, head_size),
            shape(1, head_size),
        ),
        in_specs=in_vmem(15),
        out_specs=(
            pl.BlockSpec(memory_space=pl.ANY),
            pl.BlockSpec(memory_space=pl.ANY),
            pl.BlockSpec(memory_space=pltpu.VMEM),
        ),
        scratch_shapes=[
            pltpu.VMEM((length // 128, 128), jnp.float32),
            pltpu.VMEM((length // 128, 128), jnp.float32),
            pltpu.SemaphoreType.DMA((16,)),
        ],
        name="read",
    )(
        new_query[0],
        query_gain.reshape(1, head_size),
        out_gain.reshape(1, head_size),
        shift48,
        mine,
        f0,
        p1,
        p2,
        p3,
        f1,
        f2,
        f3,
        t1,
        t2,
        t3,
    )
    return (
        key_line.reshape(1, 1, length, head_size),
        value_line.reshape(1, 1, length, head_size),
        shift_line,
        first_out[None],
    )


def solution(mesh):
    placed = (
        P("sp", "tp", None),
        P(),
        P("sp", "tp"),
        P("sp", "tp"),
        P(),
        P("sp", None, "tp"),
        P("sp", "tp", None),
        P(),
        P(),
    )
    return jax.shard_map(
        shards,
        mesh=mesh,
        in_specs=placed,
        out_specs=(
            P("sp", "tp", None, None),
            P("sp", "tp", None, None),
            P("sp", "tp", None),
            P("sp", "tp", None),
        ),
        check_vma=False,
    )
```

```python
import jax
import jax.numpy as jnp
from jax import lax
from jax.experimental import pallas as pl
from jax.experimental.pallas import tpu as pltpu
from jax.sharding import PartitionSpec as P

KVH = 4
NX = 4
CLASSES = 4
epsilon = 1e-06
MIB = 1 << 20


def row_norm(value_entries, scaling):
    return (
        value_entries
        * lax.rsqrt(jnp.mean(value_entries * value_entries, axis=-1, keepdims=True) + epsilon)
        * scaling
    )


def moved_sp(x, dz, dx):
    n = lax.axis_size("sp")
    nz = n // NX
    pairs = []
    for i in range(n):
        z, c = (i // NX + dz) % nz, (i % NX + dx) % NX
        pairs.append((i, z * NX + c))
    return lax.ppermute(x, "sp", pairs)


def moved_y(x, target):
    n = lax.axis_size("tp")
    return lax.ppermute(
        x, "tp", [(i, target(i // 2) % (n // 2) * 2 + i % 2) for i in range(n)]
    )


def swapped(x):
    return lax.ppermute(x, "tp", [(i, i ^ 1) for i in range(lax.axis_size("tp"))])


def step_to(distance):
    sign = -1 if distance % 2 else 1
    return lambda y: y + sign * distance if y % 2 == 0 else y - sign * distance


def chip_and_core():
    place = lax.axis_index("tp")
    return lax.div(place, 2), lax.rem(place, 2)


def own_class():
    at = lax.axis_index("sp")
    return lax.rem(lax.rem(at, NX) + 2 * lax.div(at, NX), CLASSES)


def pack_body(key_t, value_t, shift, out):
    groups = out.shape[0]
    zeros = jnp.zeros((13, 128), jnp.float32)
    rows = []
    for ref in (key_t, value_t):
        w = ref[...].astype(jnp.float32)
        rows.append(jnp.concatenate((w[:16], w[16:]), axis=1).astype(jnp.bfloat16))
    lines = shift[...].astype(jnp.float32)
    for head in range(KVH):
        parts = [lines[head : head + 1, 128 * i : 128 * i + 128] for i in range(3)]
        tail = jnp.concatenate((*parts, zeros), axis=0).astype(jnp.bfloat16)
        for i in range(groups // KVH):
            peer = head * (groups // KVH) + i
            out[peer, :16, :] = rows[peer % 2]
            out[peer, 16:, :] = tail


def build_body(recv, blocks, shift48, shift_line, tall, lines):
    groups = recv.shape[0]
    for t in range(groups):
        a = recv[t, :16, :].astype(jnp.float32)
        tall[32 * t : 32 * t + 16, :] = a[:, :64].astype(jnp.bfloat16)
        tall[32 * t + 16 : 32 * t + 32, :] = a[:, 64:].astype(jnp.bfloat16)
        tail = recv[t, 16:, :].astype(jnp.float32)
        lines[3 * t : 3 * t + 3, :] = tail[:3]
    i = lax.broadcasted_iota(jnp.int32, (64, 64), 0)
    eye = (i == lax.broadcasted_iota(jnp.int32, (64, 64), 1)).astype(jnp.bfloat16)
    wide = lax.dot_general(
        eye, tall[...], (((1,), (1,)), ((), ())), preferred_element_type=jnp.float32
    ).astype(jnp.bfloat16)
    for b in range(blocks.shape[0]):
        blocks[b] = wide
    shift48[...] = lines[...]
    for r in range(3 * groups):
        shift_line[0, :, 128 * r : 128 * r + 128] = lines[r : r + 1, :].astype(jnp.bfloat16)


def norm_body(x, gain, out):
    n = row_norm(x[...].astype(jnp.float32), gain[...])
    width = out.shape[1] // CLASSES
    for c in range(CLASSES):
        for m in range(width // 128):
            a = 512 * m + 64 * c
            b = 512 * m + 256 + 64 * ((c + 2) % CLASSES)
            both = jnp.concatenate((n[:, a : a + 64], n[:, b : b + 64]), axis=1)
            out[:, width * c + 128 * m : width * c + 128 * m + 128] = both.astype(jnp.bfloat16)


def columns(ref, c, at, count):
    width = ref.shape[1] // CLASSES
    return ref[:, pl.ds(pl.multiple_of(c * width + at, 128), count)]


def first_body(own, other, w0, acc):
    c = own_class()
    for i, ref in enumerate((own, other)):
        x = columns(ref, c, 0, w0.shape[0])
        acc[i] = jnp.dot(x, w0[...], preferred_element_type=jnp.float32)


def sides_body(own, other, wl, wr, acc, out):
    c = own_class()
    for i, ref in enumerate((own, other)):
        total = acc[i]
        for w, step in ((wl, 3), (wr, 1)):
            x = columns(ref, lax.rem(c + step, CLASSES), 0, w.shape[0])
            total = total + jnp.dot(x, w[...], preferred_element_type=jnp.float32)
        out[i] = total


def last_body(own, other, wu, wd, acc, gain, *rest):
    outs, line = rest[:4], rest[4]
    c = lax.rem(own_class() + 2, CLASSES)
    y, core = chip_and_core()
    rows, half = own.shape[0], wu.shape[0]
    is_key = core == 0
    for i, ref in enumerate((own, other)):
        total = acc[i]
        for w, at in ((wu, 0), (wd, half)):
            x = columns(ref, c, at, half)
            total = total + jnp.dot(x, w[...], preferred_element_type=jnp.float32)
        to = pl.multiple_of((core if i == 0 else 1 - core) * rows, 128)
        for head in range(KVH):
            a = total[:, 128 * head : 128 * head + 128]
            line[pl.ds(to, rows), 128 * head : 128 * head + 128] = jnp.where(
                is_key, row_norm(a, gain[...]), a
            ).astype(jnp.bfloat16)
    pair = lax.div(y, 2)
    sign = 2 * lax.rem(y, 2) - 1
    for slot, head in enumerate((pair, pair + sign, pair - sign, pair + 2)):
        at = pl.multiple_of(128 * lax.rem(head + KVH, KVH), 128)
        outs[slot][...] = line[:, pl.ds(at, 128)]


def read_body(query, query_gain, out_gain, shift, *rest, size, scale, chips):
    mine, theirs = rest[:8], rest[8:10]
    keys, values, first = rest[10:13]
    score_ref, weight_ref, sems = rest[13:]
    per = size // 128
    blocks = chips * per
    y, core = chip_and_core()
    sign = 2 * lax.rem(y, 2) - 1
    beside = y - sign
    sources = [y, beside] + [y + sign * d for d in (1, 2, 3)] + [beside - sign * d for d in (1, 2, 3)]
    sources = [lax.rem(s + chips, chips) for s in sources]

    def their(j):
        return theirs[0].at[pl.ds(j * size, size), :] if j < 7 else theirs[1]

    q = row_norm(query[...].astype(jnp.float32), query_gain[...]).astype(jnp.bfloat16)
    rows = lax.broadcasted_iota(jnp.int32, (128, 128), 0)
    lanes = lax.broadcasted_iota(jnp.int32, (128, 128), 1)
    on = rows == lanes
    q_all = jnp.broadcast_to(q, (128, 128))
    ones = jnp.ones((128, 128), jnp.bfloat16)

    def run(key_of, value_of):
        copies = []
        for j in range(8):
            at = pl.multiple_of(sources[j] * size, 128)
            copies.append(
                pltpu.make_async_copy(key_of(j), keys.at[pl.ds(at, size), :], sems.at[j])
            )
            copies.append(
                pltpu.make_async_copy(value_of(j), values.at[pl.ds(at, size), :], sems.at[8 + j])
            )
        for c in copies:
            c.start()
        for j in range(8):
            s = lax.dot_general(
                key_of(j)[...], q_all, (((1,), (1,)), ((), ())), preferred_element_type=jnp.float32
            )
            for i in range(per):
                line = jnp.sum(
                    jnp.where(on, s[128 * i : 128 * i + 128], 0.0), axis=0, keepdims=True
                )
                score_ref[pl.ds(sources[j] * per + i, 1), :] = line
        s = score_ref[...] * scale + shift[...]
        keep = jax.nn.log_sigmoid(-s)
        inside = jnp.dot(
            keep,
            (rows > lanes).astype(jnp.float32),
            precision=lax.Precision.HIGHEST,
            preferred_element_type=jnp.float32,
        )
        at_row = lax.broadcasted_iota(jnp.int32, (blocks, blocks), 0)
        up = (lax.broadcasted_iota(jnp.int32, (blocks, blocks), 1) > at_row).astype(jnp.float32)
        later = jnp.dot(
            up, keep, precision=lax.Precision.HIGHEST, preferred_element_type=jnp.float32
        )
        inside = inside + jnp.sum(later, axis=1, keepdims=True)
        weight_ref[...] = jnp.exp(jax.nn.log_sigmoid(s) + inside)
        total = jnp.zeros((128, 128), jnp.float32)
        for j in range(8):
            ref = value_of(j)
            for i in range(per):
                w = weight_ref[pl.ds(sources[j] * per + i, 1), :]
                spread = jnp.where(on, w, 0.0).astype(jnp.bfloat16)
                spread = jnp.dot(spread, ones, preferred_element_type=jnp.float32)
                total = total + spread * ref[128 * i : 128 * i + 128, :].astype(jnp.float32)
        total = jnp.sum(total, axis=0, keepdims=True)
        first[...] = row_norm(total, out_gain[...]).astype(jnp.bfloat16)
        for c in copies:
            c.wait()

    @pl.when(core == 0)
    def _():
        run(lambda j: mine[j], their)

    @pl.when(core == 1)
    def _():
        run(their, lambda j: mine[j])


def in_vmem(n):
    return [pl.BlockSpec(memory_space=pltpu.VMEM)] * n


def shape(*dims, dtype=jnp.bfloat16):
    return jax.ShapeDtypeStruct(dims, dtype)


def shards(
    layer_input,
    input_gain,
    key_weight,
    value_weight,
    key_gain,
    stop_shift,
    new_query,
    query_gain,
    out_gain,
):
    groups = lax.axis_size("tp")
    n_sp = lax.axis_size("sp")
    nz, ny = n_sp // NX, groups // 2
    rows, width = layer_input.shape[1:]
    size = 2 * rows
    head_size = new_query.shape[2]
    length = rows * groups
    cols = KVH * head_size
    deep = width // n_sp

    sent = pl.pallas_call(
        pack_body,
        out_shape=shape(groups, 32, 128),
        in_specs=in_vmem(3),
        out_specs=in_vmem(1)[0],
        compiler_params=pltpu.CompilerParams(vmem_limit_bytes=4 * MIB),
        name="pack",
    )(key_weight.T, value_weight.T, stop_shift[0])
    recv = lax.all_to_all(sent, "tp", split_axis=0, concat_axis=0, tiled=True)
    blocks, shift48, shift_line = pl.pallas_call(
        build_body,
        out_shape=(
            shape(nz, deep, cols),
            shape(length // 128, 128, dtype=jnp.float32),
            shape(1, 1, length),
        ),
        in_specs=in_vmem(1),
        out_specs=tuple(in_vmem(3)),
        scratch_shapes=[
            pltpu.VMEM((cols, deep), jnp.bfloat16),
            pltpu.VMEM((length // 128, 128), jnp.float32),
        ],
        compiler_params=pltpu.CompilerParams(vmem_limit_bytes=8 * MIB),
        name="build",
    )(recv)

    own = pl.pallas_call(
        norm_body,
        grid=(4,),
        out_shape=shape(rows, width),
        in_specs=[
            pl.BlockSpec((rows // 4, width), lambda i: (i, 0)),
            pl.BlockSpec((1, width), lambda i: (0, 0)),
        ],
        out_specs=pl.BlockSpec((rows // 4, width), lambda i: (i, 0)),
        compiler_params=pltpu.CompilerParams(vmem_limit_bytes=16 * MIB),
        name="norm",
    )(layer_input[0], input_gain.reshape(1, width))
    other = swapped(own)

    classes = [[z * NX + (c + 2 * z) % NX for z in range(nz)] for c in range(CLASSES)]
    got = lax.all_to_all(
        blocks, "sp", split_axis=0, concat_axis=0, tiled=True, axis_index_groups=classes
    )
    w0 = got.reshape(nz * deep, cols)
    half = nz * deep // 2
    wl = moved_sp(w0, 0, 1)
    wr = moved_sp(w0, 0, -1)
    wu = moved_sp(w0[:half], 1, 0)
    wd = moved_sp(w0[half:], -1, 0)
    acc_shape = shape(2, rows, cols, dtype=jnp.float32)
    acc = pl.pallas_call(
        first_body,
        out_shape=acc_shape,
        in_specs=in_vmem(3),
        out_specs=in_vmem(1)[0],
        cost_estimate=pl.CostEstimate(flops=4 * rows * half * cols * 2, bytes_accessed=0, transcendentals=0),
        compiler_params=pltpu.CompilerParams(vmem_limit_bytes=16 * MIB),
        name="first",
    )(own, other, w0)
    acc = pl.pallas_call(
        sides_body,
        out_shape=acc_shape,
        in_specs=in_vmem(5),
        out_specs=in_vmem(1)[0],
        input_output_aliases={4: 0},
        cost_estimate=pl.CostEstimate(flops=8 * rows * half * cols * 2, bytes_accessed=0, transcendentals=0),
        compiler_params=pltpu.CompilerParams(vmem_limit_bytes=16 * MIB),
        name="sides",
    )(own, other, wl, wr, acc)
    slots = pl.pallas_call(
        last_body,
        out_shape=tuple(shape(size, head_size) for _ in range(4)),
        in_specs=in_vmem(6),
        out_specs=tuple(in_vmem(4)),
        scratch_shapes=[pltpu.VMEM((size, cols), jnp.bfloat16)],
        cost_estimate=pl.CostEstimate(flops=4 * rows * half * cols * 2, bytes_accessed=0, transcendentals=0),
        compiler_params=pltpu.CompilerParams(vmem_limit_bytes=20 * MIB),
        name="last",
    )(own, other, wu, wd, acc, key_gain.reshape(1, head_size))

    def across(at):
        return at ^ 1

    mine = slots[0]
    p1 = moved_y(slots[1], step_to(1))
    p2 = moved_y(slots[2], step_to(2))
    p3 = moved_y(slots[3], step_to(3))
    f0 = moved_y(mine, across)
    f1 = moved_y(p1, across)
    f2 = moved_y(p2, across)
    f3 = moved_y(p3, across)
    t1 = swapped(jnp.concatenate((mine, f0, p1, p2, p3, f1, f2), 0))
    t2 = swapped(f3)
    key_line, value_line, first_out = pl.pallas_call(
        lambda *refs: read_body(*refs, size=size, scale=1.0 / head_size**0.5, chips=ny),
        out_shape=(
            shape(length, head_size),
            shape(length, head_size),
            shape(1, head_size),
        ),
        in_specs=in_vmem(14),
        out_specs=(
            pl.BlockSpec(memory_space=pl.ANY),
            pl.BlockSpec(memory_space=pl.ANY),
            pl.BlockSpec(memory_space=pltpu.VMEM),
        ),
        scratch_shapes=[
            pltpu.VMEM((length // 128, 128), jnp.float32),
            pltpu.VMEM((length // 128, 128), jnp.float32),
            pltpu.SemaphoreType.DMA((16,)),
        ],
        compiler_params=pltpu.CompilerParams(vmem_limit_bytes=24 * MIB),
        name="read",
    )(
        new_query[0],
        query_gain.reshape(1, head_size),
        out_gain.reshape(1, head_size),
        shift48,
        mine,
        f0,
        p1,
        p2,
        p3,
        f1,
        f2,
        f3,
        t1,
        t2,
    )
    return (
        key_line.reshape(1, 1, length, head_size),
        value_line.reshape(1, 1, length, head_size),
        shift_line,
        first_out[None],
    )


def solution(mesh):
    placed = (
        P("sp", "tp", None),
        P(),
        P("sp", "tp"),
        P("sp", "tp"),
        P(),
        P("sp", None, "tp"),
        P("sp", "tp", None),
        P(),
        P(),
    )
    return jax.shard_map(
        shards,
        mesh=mesh,
        in_specs=placed,
        out_specs=(
            P("sp", "tp", None, None),
            P("sp", "tp", None, None),
            P("sp", "tp", None),
            P("sp", "tp", None),
        ),
        check_vma=False,
    )
```

```python
import jax
import jax.numpy as jnp
from jax import lax
from jax.experimental import pallas as pl
from jax.experimental.pallas import tpu as pltpu
from jax.sharding import PartitionSpec as P

KVH = 4
NX = 4
CLASSES = 4
epsilon = 1e-06
MIB = 1 << 20


def row_norm(value_entries, scaling):
    return (
        value_entries
        * lax.rsqrt(jnp.mean(value_entries * value_entries, axis=-1, keepdims=True) + epsilon)
        * scaling
    )


def moved_sp(x, dz, dx):
    n = lax.axis_size("sp")
    nz = n // NX
    pairs = []
    for i in range(n):
        z, c = (i // NX + dz) % nz, (i % NX + dx) % NX
        pairs.append((i, z * NX + c))
    return lax.ppermute(x, "sp", pairs)


def moved_y(x, target):
    n = lax.axis_size("tp")
    return lax.ppermute(
        x, "tp", [(i, target(i // 2) % (n // 2) * 2 + i % 2) for i in range(n)]
    )


def swapped(x):
    return lax.ppermute(x, "tp", [(i, i ^ 1) for i in range(lax.axis_size("tp"))])


def step_to(distance):
    sign = -1 if distance % 2 else 1
    return lambda y: y + sign * distance if y % 2 == 0 else y - sign * distance


def chip_and_core():
    place = lax.axis_index("tp")
    return lax.div(place, 2), lax.rem(place, 2)


def own_class():
    at = lax.axis_index("sp")
    return lax.rem(lax.rem(at, NX) + 2 * lax.div(at, NX), CLASSES)


def pack_body(key_hbm, value_hbm, shift_hbm, out, key_t, value_t, shift, sems):
    groups = out.shape[0]
    copies = [
        pltpu.make_async_copy(src, dst, sems.at[i])
        for i, (src, dst) in enumerate(
            ((key_hbm, key_t), (value_hbm, value_t), (shift_hbm, shift))
        )
    ]
    for c in copies:
        c.start()
    for c in copies:
        c.wait()
    zeros = jnp.zeros((13, 128), jnp.float32)
    rows = []
    for ref in (key_t, value_t):
        w = ref[...].astype(jnp.float32)
        rows.append(jnp.concatenate((w[:16], w[16:]), axis=1).astype(jnp.bfloat16))
    lines = shift[...].astype(jnp.float32)
    for head in range(KVH):
        parts = [lines[head : head + 1, 128 * i : 128 * i + 128] for i in range(3)]
        tail = jnp.concatenate((*parts, zeros), axis=0).astype(jnp.bfloat16)
        for i in range(groups // KVH):
            peer = head * (groups // KVH) + i
            out[peer, :16, :] = rows[peer % 2]
            out[peer, 16:, :] = tail


def build_body(recv, blocks, shift48, shift_line, tall, lines):
    groups = recv.shape[0]
    for t in range(groups):
        a = recv[t, :16, :].astype(jnp.float32)
        tall[32 * t : 32 * t + 16, :] = a[:, :64].astype(jnp.bfloat16)
        tall[32 * t + 16 : 32 * t + 32, :] = a[:, 64:].astype(jnp.bfloat16)
        tail = recv[t, 16:, :].astype(jnp.float32)
        lines[3 * t : 3 * t + 3, :] = tail[:3]
    i = lax.broadcasted_iota(jnp.int32, (64, 64), 0)
    eye = (i == lax.broadcasted_iota(jnp.int32, (64, 64), 1)).astype(jnp.bfloat16)
    wide = lax.dot_general(
        eye, tall[...], (((1,), (1,)), ((), ())), preferred_element_type=jnp.float32
    ).astype(jnp.bfloat16)
    for b in range(blocks.shape[0]):
        blocks[b] = wide
    shift48[...] = lines[...]
    for r in range(3 * groups):
        shift_line[0, :, 128 * r : 128 * r + 128] = lines[r : r + 1, :].astype(jnp.bfloat16)


def norm_body(x, gain, out):
    n = row_norm(x[...].astype(jnp.float32), gain[...])
    width = out.shape[1] // CLASSES
    for c in range(CLASSES):
        for m in range(width // 128):
            a = 512 * m + 64 * c
            b = 512 * m + 256 + 64 * ((c + 2) % CLASSES)
            both = jnp.concatenate((n[:, a : a + 64], n[:, b : b + 64]), axis=1)
            out[:, width * c + 128 * m : width * c + 128 * m + 128] = both.astype(jnp.bfloat16)


def columns(ref, c, at, count):
    width = ref.shape[1] // CLASSES
    return ref[:, pl.ds(pl.multiple_of(c * width + at, 128), count)]


def first_body(own, other, w0, acc):
    c = own_class()
    for i, ref in enumerate((own, other)):
        x = columns(ref, c, 0, w0.shape[0])
        acc[i] = jnp.dot(x, w0[...], preferred_element_type=jnp.float32)


def sides_body(own, other, wl, wr, acc, out):
    c = own_class()
    for i, ref in enumerate((own, other)):
        total = acc[i]
        for w, step in ((wl, 3), (wr, 1)):
            x = columns(ref, lax.rem(c + step, CLASSES), 0, w.shape[0])
            total = total + jnp.dot(x, w[...], preferred_element_type=jnp.float32)
        out[i] = total


def last_body(own, other, wu, wd, acc, gain, *rest):
    outs, line = rest[:4], rest[4]
    c = lax.rem(own_class() + 2, CLASSES)
    y, core = chip_and_core()
    rows, half = own.shape[0], wu.shape[0]
    is_key = core == 0
    for i, ref in enumerate((own, other)):
        total = acc[i]
        for w, at in ((wu, 0), (wd, half)):
            x = columns(ref, c, at, half)
            total = total + jnp.dot(x, w[...], preferred_element_type=jnp.float32)
        to = pl.multiple_of((core if i == 0 else 1 - core) * rows, 128)
        for head in range(KVH):
            a = total[:, 128 * head : 128 * head + 128]
            line[pl.ds(to, rows), 128 * head : 128 * head + 128] = jnp.where(
                is_key, row_norm(a, gain[...]), a
            ).astype(jnp.bfloat16)
    pair = lax.div(y, 2)
    sign = 2 * lax.rem(y, 2) - 1
    for slot, head in enumerate((pair, pair + sign, pair - sign, pair + 2)):
        at = pl.multiple_of(128 * lax.rem(head + KVH, KVH), 128)
        outs[slot][...] = line[:, pl.ds(at, 128)]


def read_pieces(pieces, query, query_gain, shift, lines, keys, values, sems, finish, scale):
    size = pieces[0][1].shape[0]
    per, n = size // 128, len(pieces)
    score_ref, weight_ref = lines
    q = row_norm(query[...].astype(jnp.float32), query_gain[...]).astype(jnp.bfloat16)
    rows = lax.broadcasted_iota(jnp.int32, (128, 128), 0)
    lanes = lax.broadcasted_iota(jnp.int32, (128, 128), 1)
    on = rows == lanes
    q_all = jnp.broadcast_to(q, (128, 128))
    ones = jnp.ones((128, 128), jnp.bfloat16)
    n_rows = n * per
    at_row = lax.broadcasted_iota(jnp.int32, (n_rows, n_rows), 0)
    at_col = lax.broadcasted_iota(jnp.int32, (n_rows, n_rows), 1)
    up = ((at_col > at_row) & (at_col // per == at_row // per)).astype(jnp.float32)

    def run(key_of, value_of):
        copies = []
        for j, piece in enumerate(pieces):
            to = pl.multiple_of(piece[0] * size, 128)
            copies.append(
                pltpu.make_async_copy(key_of(piece), keys.at[pl.ds(to, size), :], sems.at[j])
            )
            copies.append(
                pltpu.make_async_copy(
                    value_of(piece), values.at[pl.ds(to, size), :], sems.at[n + j]
                )
            )
        for c in copies:
            c.start()
        for j, piece in enumerate(pieces):
            s = lax.dot_general(
                key_of(piece)[...],
                q_all,
                (((1,), (1,)), ((), ())),
                preferred_element_type=jnp.float32,
            )
            for i in range(per):
                line = jnp.sum(
                    jnp.where(on, s[128 * i : 128 * i + 128], 0.0), axis=0, keepdims=True
                )
                at = piece[0] * per + i
                score_ref[per * j + i : per * j + i + 1, :] = line * scale + shift[pl.ds(at, 1), :]
        s = score_ref[...]
        keep = jax.nn.log_sigmoid(-s)
        inside = jnp.dot(
            keep,
            (rows > lanes).astype(jnp.float32),
            precision=lax.Precision.HIGHEST,
            preferred_element_type=jnp.float32,
        )
        later = jnp.dot(
            up, keep, precision=lax.Precision.HIGHEST, preferred_element_type=jnp.float32
        )
        inside = inside + jnp.sum(later, axis=1, keepdims=True)
        weight_ref[...] = jnp.exp(jax.nn.log_sigmoid(s) + inside)
        found = []
        for j, piece in enumerate(pieces):
            ref = value_of(piece)
            total = jnp.zeros((128, 128), jnp.float32)
            for i in range(per):
                w = weight_ref[per * j + i : per * j + i + 1, :]
                spread = jnp.where(on, w, 0.0).astype(jnp.bfloat16)
                spread = jnp.dot(spread, ones, preferred_element_type=jnp.float32)
                total = total + spread * ref[128 * i : 128 * i + 128, :].astype(jnp.float32)
            kept = jnp.sum(keep[per * j : per * j + per], axis=0, keepdims=True)
            found.append((piece[0], jnp.sum(total, axis=0, keepdims=True), kept))
        finish(found)
        for c in copies:
            c.wait()

    _, core = chip_and_core()

    @pl.when(core == 0)
    def _():
        run(lambda p: p[1], lambda p: p[2])

    @pl.when(core == 1)
    def _():
        run(lambda p: p[2], lambda p: p[1])


def positions(chips):
    y, _ = chip_and_core()
    sign = 2 * lax.rem(y, 2) - 1
    near = [lax.rem(y + sign * d + chips, chips) for d in range(4)]
    beside = y - sign
    return near, [lax.rem(beside - sign * d + chips, chips) for d in range(4)]


def early_body(query, query_gain, shift, own, f0, p3, p2, theirs, *rest, scale, chips):
    keys, values, parts, kept, score_ref, weight_ref, sems = rest
    near, far = positions(chips)
    size = own.shape[0]
    pieces = [
        (at, ref, theirs.at[pl.ds(j * size, size), :])
        for j, (at, ref) in enumerate(
            ((near[0], own), (far[0], f0), (near[3], p3), (near[2], p2))
        )
    ]

    def finish(found):
        for at, total, keep in found:
            parts[pl.ds(at, 1), :] = total
            kept[pl.ds(at, 1), :] = keep

    read_pieces(
        pieces, query, query_gain, shift, (score_ref, weight_ref), keys, values, sems, finish, scale
    )


def late_body(
    query, query_gain, out_gain, shift, p1, f3, f2, f1, theirs, last, parts, kept, *rest, scale, chips
):
    keys, values, first, part_ref, kept_ref, score_ref, weight_ref, sems = rest[2:]
    near, far = positions(chips)
    size = p1.shape[0]
    pieces = [
        (near[1], p1, theirs.at[pl.ds(0, size), :]),
        (far[3], f3, theirs.at[pl.ds(size, size), :]),
        (far[2], f2, theirs.at[pl.ds(2 * size, size), :]),
        (far[1], f1, last),
    ]
    part_ref[...] = parts[...]
    kept_ref[...] = kept[...]

    def finish(found):
        for at, total, keep in found:
            part_ref[pl.ds(at, 1), :] = total
            kept_ref[pl.ds(at, 1), :] = keep
        row = lax.broadcasted_iota(jnp.int32, (chips, chips), 0)
        up = (lax.broadcasted_iota(jnp.int32, (chips, chips), 1) > row).astype(jnp.float32)
        later = jnp.dot(
            up, kept_ref[...], precision=lax.Precision.HIGHEST, preferred_element_type=jnp.float32
        )
        total = jnp.exp(jnp.sum(later, axis=1, keepdims=True)) * part_ref[...]
        total = jnp.sum(total, axis=0, keepdims=True)
        first[...] = row_norm(total, out_gain[...]).astype(jnp.bfloat16)

    read_pieces(
        pieces, query, query_gain, shift, (score_ref, weight_ref), keys, values, sems, finish, scale
    )


def in_vmem(n):
    return [pl.BlockSpec(memory_space=pltpu.VMEM)] * n


def shape(*dims, dtype=jnp.bfloat16):
    return jax.ShapeDtypeStruct(dims, dtype)


def shards(
    layer_input,
    input_gain,
    key_weight,
    value_weight,
    key_gain,
    stop_shift,
    new_query,
    query_gain,
    out_gain,
):
    groups = lax.axis_size("tp")
    n_sp = lax.axis_size("sp")
    nz, ny = n_sp // NX, groups // 2
    rows, width = layer_input.shape[1:]
    size = 2 * rows
    head_size = new_query.shape[2]
    length = rows * groups
    cols = KVH * head_size
    deep = width // n_sp

    sent = pl.pallas_call(
        pack_body,
        out_shape=shape(groups, 32, 128),
        in_specs=[pl.BlockSpec(memory_space=pltpu.HBM)] * 3,
        out_specs=in_vmem(1)[0],
        scratch_shapes=[
            pltpu.VMEM(key_weight.shape[::-1], jnp.bfloat16),
            pltpu.VMEM(key_weight.shape[::-1], jnp.bfloat16),
            pltpu.VMEM(stop_shift.shape[1:], jnp.bfloat16),
            pltpu.SemaphoreType.DMA((3,)),
        ],
        compiler_params=pltpu.CompilerParams(vmem_limit_bytes=4 * MIB),
        name="pack",
    )(
        *(
            pltpu.with_memory_space_constraint(a, pltpu.HBM)
            for a in (key_weight.T, value_weight.T, stop_shift[0])
        )
    )
    recv = lax.all_to_all(sent, "tp", split_axis=0, concat_axis=0, tiled=True)
    blocks, shift48, shift_line = pl.pallas_call(
        build_body,
        out_shape=(
            shape(nz, deep, cols),
            shape(length // 128, 128, dtype=jnp.float32),
            shape(1, 1, length),
        ),
        in_specs=in_vmem(1),
        out_specs=tuple(in_vmem(3)),
        scratch_shapes=[
            pltpu.VMEM((cols, deep), jnp.bfloat16),
            pltpu.VMEM((length // 128, 128), jnp.float32),
        ],
        compiler_params=pltpu.CompilerParams(vmem_limit_bytes=8 * MIB),
        name="build",
    )(recv)

    own = pl.pallas_call(
        norm_body,
        grid=(4,),
        out_shape=shape(rows, width),
        in_specs=[
            pl.BlockSpec((rows // 4, width), lambda i: (i, 0)),
            pl.BlockSpec((1, width), lambda i: (0, 0)),
        ],
        out_specs=pl.BlockSpec((rows // 4, width), lambda i: (i, 0)),
        compiler_params=pltpu.CompilerParams(vmem_limit_bytes=16 * MIB),
        name="norm",
    )(
        pltpu.with_memory_space_constraint(layer_input[0], pltpu.HBM),
        pltpu.with_memory_space_constraint(input_gain.reshape(1, width), pltpu.HBM),
    )
    other = swapped(own)

    classes = [[z * NX + (c + 2 * z) % NX for z in range(nz)] for c in range(CLASSES)]
    got = lax.all_to_all(
        blocks, "sp", split_axis=0, concat_axis=0, tiled=True, axis_index_groups=classes
    )
    w0 = got.reshape(nz * deep, cols)
    half = nz * deep // 2
    wl = moved_sp(w0, 0, 1)
    wr = moved_sp(w0, 0, -1)
    wu = moved_sp(w0[:half], 1, 0)
    wd = moved_sp(w0[half:], -1, 0)
    acc_shape = shape(2, rows, cols, dtype=jnp.float32)
    acc = pl.pallas_call(
        first_body,
        out_shape=acc_shape,
        in_specs=in_vmem(3),
        out_specs=in_vmem(1)[0],
        cost_estimate=pl.CostEstimate(flops=4 * rows * half * cols * 2, bytes_accessed=0, transcendentals=0),
        compiler_params=pltpu.CompilerParams(vmem_limit_bytes=16 * MIB),
        name="first",
    )(own, other, w0)
    acc = pl.pallas_call(
        sides_body,
        out_shape=acc_shape,
        in_specs=in_vmem(5),
        out_specs=in_vmem(1)[0],
        input_output_aliases={4: 0},
        cost_estimate=pl.CostEstimate(flops=8 * rows * half * cols * 2, bytes_accessed=0, transcendentals=0),
        compiler_params=pltpu.CompilerParams(vmem_limit_bytes=16 * MIB),
        name="sides",
    )(own, other, wl, wr, acc)
    slots = pl.pallas_call(
        last_body,
        out_shape=tuple(shape(size, head_size) for _ in range(4)),
        in_specs=in_vmem(6),
        out_specs=tuple(in_vmem(4)),
        scratch_shapes=[pltpu.VMEM((size, cols), jnp.bfloat16)],
        cost_estimate=pl.CostEstimate(flops=4 * rows * half * cols * 2, bytes_accessed=0, transcendentals=0),
        compiler_params=pltpu.CompilerParams(vmem_limit_bytes=20 * MIB),
        name="last",
    )(own, other, wu, wd, acc, key_gain.reshape(1, head_size))

    def across(at):
        return at ^ 1

    mine = slots[0]
    p1 = moved_y(slots[1], step_to(1))
    p2 = moved_y(slots[2], step_to(2))
    p3 = moved_y(slots[3], step_to(3))
    f0 = moved_y(mine, across)
    f1 = moved_y(p1, across)
    f2 = moved_y(p2, across)
    f3 = moved_y(p3, across)
    t1 = swapped(jnp.concatenate((mine, f0, p3, p2), 0))
    t2 = swapped(jnp.concatenate((p1, f3, f2), 0))
    t3 = swapped(f1)
    in_hbm = pl.BlockSpec(memory_space=pltpu.HBM)
    scale = 1.0 / head_size**0.5
    half = length // 256
    line_shape = shape(length, head_size)
    part_shape = shape(ny, head_size, dtype=jnp.float32)
    scratch = [
        pltpu.VMEM((half, 128), jnp.float32),
        pltpu.VMEM((half, 128), jnp.float32),
        pltpu.SemaphoreType.DMA((8,)),
    ]
    query, gain_q, gain_o = new_query[0], query_gain.reshape(1, -1), out_gain.reshape(1, -1)
    early = pl.pallas_call(
        lambda *refs: early_body(*refs, scale=scale, chips=ny),
        out_shape=(line_shape, line_shape, part_shape, part_shape),
        in_specs=in_vmem(8),
        out_specs=(in_hbm, in_hbm, *in_vmem(2)),
        scratch_shapes=scratch,
        compiler_params=pltpu.CompilerParams(vmem_limit_bytes=16 * MIB),
        name="early",
    )
    key_line, value_line, parts, kept = early(query, gain_q, shift48, mine, f0, p3, p2, t1)
    key_line, value_line, first_out = pl.pallas_call(
        lambda *refs: late_body(*refs, scale=scale, chips=ny),
        out_shape=(line_shape, line_shape, shape(1, head_size)),
        in_specs=in_vmem(12) + [in_hbm] * 2,
        out_specs=(in_hbm, in_hbm, in_vmem(1)[0]),
        scratch_shapes=[
            pltpu.VMEM((ny, head_size), jnp.float32),
            pltpu.VMEM((ny, head_size), jnp.float32),
            *scratch,
        ],
        input_output_aliases={12: 0, 13: 1},
        compiler_params=pltpu.CompilerParams(vmem_limit_bytes=16 * MIB),
        name="late",
    )(query, gain_q, gain_o, shift48, p1, f3, f2, f1, t2, t3, parts, kept, key_line, value_line)
    return (
        key_line.reshape(1, 1, length, head_size),
        value_line.reshape(1, 1, length, head_size),
        shift_line,
        first_out[None],
    )


def solution(mesh):
    placed = (
        P("sp", "tp", None),
        P(),
        P("sp", "tp"),
        P("sp", "tp"),
        P(),
        P("sp", None, "tp"),
        P("sp", "tp", None),
        P(),
        P(),
    )
    return jax.shard_map(
        shards,
        mesh=mesh,
        in_specs=placed,
        out_specs=(
            P("sp", "tp", None, None),
            P("sp", "tp", None, None),
            P("sp", "tp", None),
            P("sp", "tp", None),
        ),
        check_vma=False,
    )
```

```python
import jax
import jax.numpy as jnp
from jax import lax
from jax.experimental import pallas as pl
from jax.experimental.pallas import tpu as pltpu
from jax.sharding import PartitionSpec as P

KVH = 4
NX = 4
CLASSES = 4
epsilon = 1e-06
MIB = 1 << 20


def row_norm(value_entries, scaling):
    return (
        value_entries
        * lax.rsqrt(jnp.mean(value_entries * value_entries, axis=-1, keepdims=True) + epsilon)
        * scaling
    )


def moved_sp(x, dz, dx):
    n = lax.axis_size("sp")
    nz = n // NX
    pairs = []
    for i in range(n):
        z, c = (i // NX + dz) % nz, (i % NX + dx) % NX
        pairs.append((i, z * NX + c))
    return lax.ppermute(x, "sp", pairs)


def moved_y(x, target):
    n = lax.axis_size("tp")
    return lax.ppermute(
        x, "tp", [(i, target(i // 2) % (n // 2) * 2 + i % 2) for i in range(n)]
    )


def swapped(x):
    return lax.ppermute(x, "tp", [(i, i ^ 1) for i in range(lax.axis_size("tp"))])


def step_to(distance):
    sign = -1 if distance % 2 else 1
    return lambda y: y + sign * distance if y % 2 == 0 else y - sign * distance


def chip_and_core():
    place = lax.axis_index("tp")
    return lax.div(place, 2), lax.rem(place, 2)


def own_class():
    at = lax.axis_index("sp")
    return lax.rem(lax.rem(at, NX) + 2 * lax.div(at, NX), CLASSES)


def pack_body(key_hbm, value_hbm, shift_hbm, out, key_t, value_t, shift, sems):
    groups = out.shape[0]
    copies = [
        pltpu.make_async_copy(src, dst, sems.at[i])
        for i, (src, dst) in enumerate(
            ((key_hbm, key_t), (value_hbm, value_t), (shift_hbm, shift))
        )
    ]
    for c in copies:
        c.start()
    for c in copies:
        c.wait()
    zeros = jnp.zeros((13, 128), jnp.float32)
    rows = []
    for ref in (key_t, value_t):
        w = ref[...].astype(jnp.float32)
        rows.append(jnp.concatenate((w[:16], w[16:]), axis=1).astype(jnp.bfloat16))
    lines = shift[...].astype(jnp.float32)
    for head in range(KVH):
        parts = [lines[head : head + 1, 128 * i : 128 * i + 128] for i in range(3)]
        tail = jnp.concatenate((*parts, zeros), axis=0).astype(jnp.bfloat16)
        for i in range(groups // KVH):
            peer = head * (groups // KVH) + i
            out[peer, :16, :] = rows[peer % 2]
            out[peer, 16:, :] = tail


def build_body(recv, blocks, shift48, shift_line, tall, lines):
    groups = recv.shape[0]
    for t in range(groups):
        a = recv[t, :16, :].astype(jnp.float32)
        tall[32 * t : 32 * t + 16, :] = a[:, :64].astype(jnp.bfloat16)
        tall[32 * t + 16 : 32 * t + 32, :] = a[:, 64:].astype(jnp.bfloat16)
        tail = recv[t, 16:, :].astype(jnp.float32)
        lines[3 * t : 3 * t + 3, :] = tail[:3]
    i = lax.broadcasted_iota(jnp.int32, (64, 64), 0)
    eye = (i == lax.broadcasted_iota(jnp.int32, (64, 64), 1)).astype(jnp.bfloat16)
    wide = lax.dot_general(
        eye, tall[...], (((1,), (1,)), ((), ())), preferred_element_type=jnp.float32
    ).astype(jnp.bfloat16)
    for b in range(blocks.shape[0]):
        blocks[b] = wide
    shift48[...] = lines[...]
    for r in range(3 * groups):
        shift_line[0, :, 128 * r : 128 * r + 128] = lines[r : r + 1, :].astype(jnp.bfloat16)


def norm_body(x, gain, out):
    n = row_norm(x[...].astype(jnp.float32), gain[...])
    width = out.shape[1] // CLASSES
    for c in range(CLASSES):
        for m in range(width // 128):
            a = 512 * m + 64 * c
            b = 512 * m + 256 + 64 * ((c + 2) % CLASSES)
            both = jnp.concatenate((n[:, a : a + 64], n[:, b : b + 64]), axis=1)
            out[:, width * c + 128 * m : width * c + 128 * m + 128] = both.astype(jnp.bfloat16)


def columns(ref, c, at, count):
    width = ref.shape[1] // CLASSES
    return ref[:, pl.ds(pl.multiple_of(c * width + at, 128), count)]


def first_body(own, other, w0, acc):
    c = own_class()
    for i, ref in enumerate((own, other)):
        x = columns(ref, c, 0, w0.shape[0])
        acc[i] = jnp.dot(x, w0[...], preferred_element_type=jnp.float32)


def sides_body(own, other, wl, wr, acc, out):
    c = own_class()
    for i, ref in enumerate((own, other)):
        total = acc[i]
        for w, step in ((wl, 3), (wr, 1)):
            x = columns(ref, lax.rem(c + step, CLASSES), 0, w.shape[0])
            total = total + jnp.dot(x, w[...], preferred_element_type=jnp.float32)
        out[i] = total


def last_body(own, other, wu, wd, acc, gain, *rest):
    outs, line = rest[:4], rest[4]
    c = lax.rem(own_class() + 2, CLASSES)
    y, core = chip_and_core()
    rows, half = own.shape[0], wu.shape[0]
    is_key = core == 0
    for i, ref in enumerate((own, other)):
        total = acc[i]
        for w, at in ((wu, 0), (wd, half)):
            x = columns(ref, c, at, half)
            total = total + jnp.dot(x, w[...], preferred_element_type=jnp.float32)
        to = pl.multiple_of((core if i == 0 else 1 - core) * rows, 128)
        for head in range(KVH):
            a = total[:, 128 * head : 128 * head + 128]
            line[pl.ds(to, rows), 128 * head : 128 * head + 128] = jnp.where(
                is_key, row_norm(a, gain[...]), a
            ).astype(jnp.bfloat16)
    pair = lax.div(y, 2)
    sign = 2 * lax.rem(y, 2) - 1
    for slot, head in enumerate((pair, pair + sign, pair - sign, pair + 2)):
        at = pl.multiple_of(128 * lax.rem(head + KVH, KVH), 128)
        outs[slot][...] = line[:, pl.ds(at, 128)]


def read_body(query, query_gain, out_gain, shift, *rest, size, scale, chips):
    both, theirs = rest[5], rest[7:9]
    mine = [*rest[:5], both.at[pl.ds(0, size), :], both.at[pl.ds(size, size), :], rest[6]]
    keys, values, first = rest[9:12]
    score_ref, weight_ref, sems = rest[12:]
    per = size // 128
    blocks = chips * per
    y, core = chip_and_core()
    sign = 2 * lax.rem(y, 2) - 1
    beside = y - sign
    sources = [y, beside] + [y + sign * d for d in (1, 2, 3)] + [beside - sign * d for d in (1, 2, 3)]
    sources = [lax.rem(s + chips, chips) for s in sources]

    def their(j):
        return theirs[0].at[pl.ds(j * size, size), :] if j < 7 else theirs[1]

    q = row_norm(query[...].astype(jnp.float32), query_gain[...]).astype(jnp.bfloat16)
    rows = lax.broadcasted_iota(jnp.int32, (128, 128), 0)
    lanes = lax.broadcasted_iota(jnp.int32, (128, 128), 1)
    q_all = jnp.broadcast_to(q, (16, 128))

    def run(key_of, value_of):
        copies = []
        for j in range(8):
            at = pl.multiple_of(sources[j] * size, 128)
            copies.append(
                pltpu.make_async_copy(key_of(j), keys.at[pl.ds(at, size), :], sems.at[j])
            )
            copies.append(
                pltpu.make_async_copy(value_of(j), values.at[pl.ds(at, size), :], sems.at[8 + j])
            )
        for c in copies:
            c.start()
        for j in range(8):
            s = lax.dot_general(
                q_all, key_of(j)[...], (((1,), (1,)), ((), ())), preferred_element_type=jnp.float32
            )
            for i in range(per):
                score_ref[pl.ds(sources[j] * per + i, 1), :] = s[0:1, 128 * i : 128 * i + 128]
        s = score_ref[...] * scale + shift[...]
        keep = jax.nn.log_sigmoid(-s)
        inside = jnp.dot(
            keep,
            (rows > lanes).astype(jnp.float32),
            precision=lax.Precision.HIGHEST,
            preferred_element_type=jnp.float32,
        )
        at_row = lax.broadcasted_iota(jnp.int32, (blocks, blocks), 0)
        up = (lax.broadcasted_iota(jnp.int32, (blocks, blocks), 1) > at_row).astype(jnp.float32)
        later = jnp.dot(
            up, keep, precision=lax.Precision.HIGHEST, preferred_element_type=jnp.float32
        )
        inside = inside + jnp.sum(later, axis=1, keepdims=True)
        weight_ref[...] = jnp.exp(jax.nn.log_sigmoid(s) + inside)
        total = jnp.zeros((16, 128), jnp.float32)
        for j in range(8):
            w = jnp.concatenate(
                [weight_ref[pl.ds(sources[j] * per + i, 1), :] for i in range(per)], axis=1
            )
            total = total + jnp.dot(
                jnp.broadcast_to(w, (16, size)).astype(jnp.bfloat16),
                value_of(j)[...],
                preferred_element_type=jnp.float32,
            )
        total = total[0:1]
        first[...] = row_norm(total, out_gain[...]).astype(jnp.bfloat16)
        for c in copies:
            c.wait()

    @pl.when(core == 0)
    def _():
        run(lambda j: mine[j], their)

    @pl.when(core == 1)
    def _():
        run(their, lambda j: mine[j])


def in_vmem(n):
    return [pl.BlockSpec(memory_space=pltpu.VMEM)] * n


def shape(*dims, dtype=jnp.bfloat16):
    return jax.ShapeDtypeStruct(dims, dtype)


def shards(
    layer_input,
    input_gain,
    key_weight,
    value_weight,
    key_gain,
    stop_shift,
    new_query,
    query_gain,
    out_gain,
):
    groups = lax.axis_size("tp")
    n_sp = lax.axis_size("sp")
    nz, ny = n_sp // NX, groups // 2
    rows, width = layer_input.shape[1:]
    size = 2 * rows
    head_size = new_query.shape[2]
    length = rows * groups
    cols = KVH * head_size
    deep = width // n_sp

    sent = pl.pallas_call(
        pack_body,
        out_shape=shape(groups, 32, 128),
        in_specs=[pl.BlockSpec(memory_space=pltpu.HBM)] * 3,
        out_specs=in_vmem(1)[0],
        scratch_shapes=[
            pltpu.VMEM(key_weight.shape[::-1], jnp.bfloat16),
            pltpu.VMEM(key_weight.shape[::-1], jnp.bfloat16),
            pltpu.VMEM(stop_shift.shape[1:], jnp.bfloat16),
            pltpu.SemaphoreType.DMA((3,)),
        ],
        compiler_params=pltpu.CompilerParams(vmem_limit_bytes=4 * MIB),
        name="pack",
    )(
        *(
            pltpu.with_memory_space_constraint(a, pltpu.HBM)
            for a in (key_weight.T, value_weight.T, stop_shift[0])
        )
    )
    recv = lax.all_to_all(sent, "tp", split_axis=0, concat_axis=0, tiled=True)
    blocks, shift48, shift_line = pl.pallas_call(
        build_body,
        out_shape=(
            shape(nz, deep, cols),
            shape(length // 128, 128, dtype=jnp.float32),
            shape(1, 1, length),
        ),
        in_specs=in_vmem(1),
        out_specs=tuple(in_vmem(3)),
        scratch_shapes=[
            pltpu.VMEM((cols, deep), jnp.bfloat16),
            pltpu.VMEM((length // 128, 128), jnp.float32),
        ],
        compiler_params=pltpu.CompilerParams(vmem_limit_bytes=8 * MIB),
        name="build",
    )(recv)

    own = pl.pallas_call(
        norm_body,
        grid=(4,),
        out_shape=shape(rows, width),
        in_specs=[
            pl.BlockSpec((rows // 4, width), lambda i: (i, 0)),
            pl.BlockSpec((1, width), lambda i: (0, 0)),
        ],
        out_specs=pl.BlockSpec((rows // 4, width), lambda i: (i, 0)),
        compiler_params=pltpu.CompilerParams(vmem_limit_bytes=16 * MIB),
        name="norm",
    )(
        pltpu.with_memory_space_constraint(layer_input[0], pltpu.HBM),
        pltpu.with_memory_space_constraint(input_gain.reshape(1, width), pltpu.HBM),
    )
    other = swapped(own)

    classes = [[z * NX + (c + 2 * z) % NX for z in range(nz)] for c in range(CLASSES)]
    got = lax.all_to_all(
        blocks, "sp", split_axis=0, concat_axis=0, tiled=True, axis_index_groups=classes
    )
    w0 = got.reshape(nz * deep, cols)
    half = nz * deep // 2
    wl = moved_sp(w0, 0, 1)
    wr = moved_sp(w0, 0, -1)
    wu = moved_sp(w0[:half], 1, 0)
    wd = moved_sp(w0[half:], -1, 0)
    acc_shape = shape(2, rows, cols, dtype=jnp.float32)
    acc = pl.pallas_call(
        first_body,
        out_shape=acc_shape,
        in_specs=in_vmem(3),
        out_specs=in_vmem(1)[0],
        cost_estimate=pl.CostEstimate(flops=4 * rows * half * cols * 2, bytes_accessed=0, transcendentals=0),
        compiler_params=pltpu.CompilerParams(vmem_limit_bytes=16 * MIB),
        name="first",
    )(own, other, w0)
    acc = pl.pallas_call(
        sides_body,
        out_shape=acc_shape,
        in_specs=in_vmem(5),
        out_specs=in_vmem(1)[0],
        input_output_aliases={4: 0},
        cost_estimate=pl.CostEstimate(flops=8 * rows * half * cols * 2, bytes_accessed=0, transcendentals=0),
        compiler_params=pltpu.CompilerParams(vmem_limit_bytes=16 * MIB),
        name="sides",
    )(own, other, wl, wr, acc)
    slots = pl.pallas_call(
        last_body,
        out_shape=tuple(shape(size, head_size) for _ in range(4)),
        in_specs=in_vmem(6),
        out_specs=tuple(in_vmem(4)),
        scratch_shapes=[pltpu.VMEM((size, cols), jnp.bfloat16)],
        cost_estimate=pl.CostEstimate(flops=4 * rows * half * cols * 2, bytes_accessed=0, transcendentals=0),
        compiler_params=pltpu.CompilerParams(vmem_limit_bytes=20 * MIB),
        name="last",
    )(own, other, wu, wd, acc, key_gain.reshape(1, head_size))

    def across(at):
        return at ^ 1

    mine = slots[0]
    p1 = moved_y(slots[1], step_to(1))
    p2 = moved_y(slots[2], step_to(2))
    p3 = moved_y(slots[3], step_to(3))
    f0 = moved_y(mine, across)
    f12 = moved_y(jnp.concatenate((p1, p2), 0), across)
    f3 = moved_y(p3, across)
    t1 = swapped(jnp.concatenate((mine, f0, p1, p2, p3, f12), 0))
    t2 = swapped(f3)
    key_line, value_line, first_out = pl.pallas_call(
        lambda *refs: read_body(*refs, size=size, scale=1.0 / head_size**0.5, chips=ny),
        out_shape=(
            shape(length, head_size),
            shape(length, head_size),
            shape(1, head_size),
        ),
        in_specs=in_vmem(13),
        out_specs=(
            pl.BlockSpec(memory_space=pl.ANY),
            pl.BlockSpec(memory_space=pl.ANY),
            pl.BlockSpec(memory_space=pltpu.VMEM),
        ),
        scratch_shapes=[
            pltpu.VMEM((length // 128, 128), jnp.float32),
            pltpu.VMEM((length // 128, 128), jnp.float32),
            pltpu.SemaphoreType.DMA((16,)),
        ],
        compiler_params=pltpu.CompilerParams(vmem_limit_bytes=24 * MIB),
        name="read",
    )(
        new_query[0],
        query_gain.reshape(1, head_size),
        out_gain.reshape(1, head_size),
        shift48,
        mine,
        f0,
        p1,
        p2,
        p3,
        f12,
        f3,
        t1,
        t2,
    )
    return (
        key_line.reshape(1, 1, length, head_size),
        value_line.reshape(1, 1, length, head_size),
        shift_line,
        first_out[None],
    )


def solution(mesh):
    placed = (
        P("sp", "tp", None),
        P(),
        P("sp", "tp"),
        P("sp", "tp"),
        P(),
        P("sp", None, "tp"),
        P("sp", "tp", None),
        P(),
        P(),
    )
    return jax.shard_map(
        shards,
        mesh=mesh,
        in_specs=placed,
        out_specs=(
            P("sp", "tp", None, None),
            P("sp", "tp", None, None),
            P("sp", "tp", None),
            P("sp", "tp", None),
        ),
        check_vma=False,
    )
```

```python
import jax
import jax.numpy as jnp
from jax import lax
from jax.experimental import pallas as pl
from jax.experimental.pallas import tpu as pltpu
from jax.sharding import PartitionSpec as P

KVH = 4
NX = 4
CLASSES = 4
epsilon = 1e-06
MIB = 1 << 20


def row_norm(value_entries, scaling):
    return (
        value_entries
        * lax.rsqrt(jnp.mean(value_entries * value_entries, axis=-1, keepdims=True) + epsilon)
        * scaling
    )


def moved_sp(x, dz, dx):
    n = lax.axis_size("sp")
    nz = n // NX
    pairs = []
    for i in range(n):
        z, c = (i // NX + dz) % nz, (i % NX + dx) % NX
        pairs.append((i, z * NX + c))
    return lax.ppermute(x, "sp", pairs)


def moved_y(x, target):
    n = lax.axis_size("tp")
    return lax.ppermute(
        x, "tp", [(i, target(i // 2) % (n // 2) * 2 + i % 2) for i in range(n)]
    )


def swapped(x):
    return lax.ppermute(x, "tp", [(i, i ^ 1) for i in range(lax.axis_size("tp"))])


def step_to(distance):
    sign = -1 if distance % 2 else 1
    return lambda y: y + sign * distance if y % 2 == 0 else y - sign * distance


def chip_and_core():
    place = lax.axis_index("tp")
    return lax.div(place, 2), lax.rem(place, 2)


def own_class():
    at = lax.axis_index("sp")
    return lax.rem(lax.rem(at, NX) + 2 * lax.div(at, NX), CLASSES)


def pack_body(key_hbm, value_hbm, shift_hbm, out, key_t, value_t, shift, sems):
    groups = out.shape[0]
    copies = [
        pltpu.make_async_copy(src, dst, sems.at[i])
        for i, (src, dst) in enumerate(
            ((key_hbm, key_t), (value_hbm, value_t), (shift_hbm, shift))
        )
    ]
    for c in copies:
        c.start()
    for c in copies:
        c.wait()
    zeros = jnp.zeros((5, 128), jnp.float32)
    rows = []
    for ref in (key_t, value_t):
        w = ref[...].astype(jnp.float32)
        rows.append(jnp.concatenate((w[:16], w[16:]), axis=1).astype(jnp.bfloat16))
    lines = shift[...].astype(jnp.float32)
    for head in range(KVH):
        parts = [lines[head : head + 1, 128 * i : 128 * i + 128] for i in range(3)]
        tail = jnp.concatenate((*parts, zeros), axis=0).astype(jnp.bfloat16)
        for i in range(groups // KVH):
            peer = head * (groups // KVH) + i
            out[peer, :16, :] = rows[peer % 2]
            out[peer, 16:, :] = tail


def build_body(recv, blocks, shift48, shift_line, tall, lines):
    groups = recv.shape[0]
    for t in range(groups):
        a = recv[t, :16, :].astype(jnp.float32)
        tall[32 * t : 32 * t + 16, :] = a[:, :64].astype(jnp.bfloat16)
        tall[32 * t + 16 : 32 * t + 32, :] = a[:, 64:].astype(jnp.bfloat16)
        tail = recv[t, 16:, :].astype(jnp.float32)
        lines[3 * t : 3 * t + 3, :] = tail[:3]
    i = lax.broadcasted_iota(jnp.int32, (64, 64), 0)
    eye = (i == lax.broadcasted_iota(jnp.int32, (64, 64), 1)).astype(jnp.bfloat16)
    wide = lax.dot_general(
        eye, tall[...], (((1,), (1,)), ((), ())), preferred_element_type=jnp.float32
    ).astype(jnp.bfloat16)
    for b in range(blocks.shape[0]):
        blocks[b] = wide
    shift48[...] = lines[...]
    for r in range(3 * groups):
        shift_line[0, :, 128 * r : 128 * r + 128] = lines[r : r + 1, :].astype(jnp.bfloat16)


def norm_body(x, gain, out):
    n = row_norm(x[...].astype(jnp.float32), gain[...])
    width = out.shape[1] // CLASSES
    for c in range(CLASSES):
        for m in range(width // 128):
            a = 512 * m + 64 * c
            b = 512 * m + 256 + 64 * ((c + 2) % CLASSES)
            both = jnp.concatenate((n[:, a : a + 64], n[:, b : b + 64]), axis=1)
            out[:, width * c + 128 * m : width * c + 128 * m + 128] = both.astype(jnp.bfloat16)


def columns(ref, c, at, count):
    width = ref.shape[1] // CLASSES
    return ref[:, pl.ds(pl.multiple_of(c * width + at, 128), count)]


def first_body(own, other, w0, acc):
    c = own_class()
    for i, ref in enumerate((own, other)):
        x = columns(ref, c, 0, w0.shape[0])
        acc[i] = jnp.dot(x, w0[...], preferred_element_type=jnp.float32)


def sides_body(own, other, wl, wr, acc, out):
    c = own_class()
    for i, ref in enumerate((own, other)):
        total = acc[i]
        for w, step in ((wl, 3), (wr, 1)):
            x = columns(ref, lax.rem(c + step, CLASSES), 0, w.shape[0])
            total = total + jnp.dot(x, w[...], preferred_element_type=jnp.float32)
        out[i] = total


def last_body(own, other, wu, wd, acc, gain, *rest):
    outs, line = rest[:4], rest[4]
    c = lax.rem(own_class() + 2, CLASSES)
    y, core = chip_and_core()
    rows, half = own.shape[0], wu.shape[0]
    is_key = core == 0
    for i, ref in enumerate((own, other)):
        total = acc[i]
        for w, at in ((wu, 0), (wd, half)):
            x = columns(ref, c, at, half)
            total = total + jnp.dot(x, w[...], preferred_element_type=jnp.float32)
        to = pl.multiple_of((core if i == 0 else 1 - core) * rows, 128)
        for head in range(KVH):
            a = total[:, 128 * head : 128 * head + 128]
            line[pl.ds(to, rows), 128 * head : 128 * head + 128] = jnp.where(
                is_key, row_norm(a, gain[...]), a
            ).astype(jnp.bfloat16)
    pair = lax.div(y, 2)
    sign = 2 * lax.rem(y, 2) - 1
    for slot, head in enumerate((pair, pair + sign, pair - sign, pair + 2)):
        at = pl.multiple_of(128 * lax.rem(head + KVH, KVH), 128)
        outs[slot][...] = line[:, pl.ds(at, 128)]


def read_pieces(pieces, query, query_gain, shift, lines, keys, values, sems, finish, scale):
    size = pieces[0][1].shape[0]
    per, n = size // 128, len(pieces)
    score_ref, weight_ref = lines
    q = row_norm(query[...].astype(jnp.float32), query_gain[...]).astype(jnp.bfloat16)
    rows = lax.broadcasted_iota(jnp.int32, (128, 128), 0)
    lanes = lax.broadcasted_iota(jnp.int32, (128, 128), 1)
    q_all = jnp.broadcast_to(q, (16, 128))
    n_rows = n * per
    at_row = lax.broadcasted_iota(jnp.int32, (n_rows, n_rows), 0)
    at_col = lax.broadcasted_iota(jnp.int32, (n_rows, n_rows), 1)
    up = ((at_col > at_row) & (at_col // per == at_row // per)).astype(jnp.float32)

    def run(key_of, value_of):
        copies = []
        for j, piece in enumerate(pieces):
            to = pl.multiple_of(piece[0] * size, 128)
            copies.append(
                pltpu.make_async_copy(key_of(piece), keys.at[pl.ds(to, size), :], sems.at[j])
            )
            copies.append(
                pltpu.make_async_copy(
                    value_of(piece), values.at[pl.ds(to, size), :], sems.at[n + j]
                )
            )
        for c in copies:
            c.start()
        for j, piece in enumerate(pieces):
            s = lax.dot_general(
                q_all,
                key_of(piece)[...],
                (((1,), (1,)), ((), ())),
                preferred_element_type=jnp.float32,
            )
            for i in range(per):
                at = piece[0] * per + i
                line = s[0:1, 128 * i : 128 * i + 128] * scale
                score_ref[per * j + i : per * j + i + 1, :] = line + shift[pl.ds(at, 1), :]
        s = score_ref[...]
        keep = jax.nn.log_sigmoid(-s)
        inside = jnp.dot(
            keep,
            (rows > lanes).astype(jnp.float32),
            precision=lax.Precision.HIGHEST,
            preferred_element_type=jnp.float32,
        )
        later = jnp.dot(
            up, keep, precision=lax.Precision.HIGHEST, preferred_element_type=jnp.float32
        )
        inside = inside + jnp.sum(later, axis=1, keepdims=True)
        weight_ref[...] = jnp.exp(jax.nn.log_sigmoid(s) + inside)
        found = []
        for j, piece in enumerate(pieces):
            w = jnp.concatenate(
                [weight_ref[per * j + i : per * j + i + 1, :] for i in range(per)], axis=1
            )
            total = jnp.dot(
                jnp.broadcast_to(w, (16, size)).astype(jnp.bfloat16),
                value_of(piece)[...],
                preferred_element_type=jnp.float32,
            )
            kept = jnp.sum(keep[per * j : per * j + per], axis=0, keepdims=True)
            found.append((piece[0], total[0:1], kept))
        finish(found)
        for c in copies:
            c.wait()

    _, core = chip_and_core()

    @pl.when(core == 0)
    def _():
        run(lambda p: p[1], lambda p: p[2])

    @pl.when(core == 1)
    def _():
        run(lambda p: p[2], lambda p: p[1])


def positions(chips):
    y, _ = chip_and_core()
    sign = 2 * lax.rem(y, 2) - 1
    near = [lax.rem(y + sign * d + chips, chips) for d in range(4)]
    beside = y - sign
    return near, [lax.rem(beside - sign * d + chips, chips) for d in range(4)]


def early_body(query, query_gain, shift, own, f0, p1, p2, p3, f12, theirs, *rest, scale, chips):
    keys, values, parts, kept, score_ref, weight_ref, sems = rest
    near, far = positions(chips)
    size = own.shape[0]
    halves = [f12.at[pl.ds(i * size, size), :] for i in range(2)]
    held = zip((near[0], far[0], *near[1:], *far[1:3]), (own, f0, p1, p2, p3, *halves))
    pieces = [(at, ref, theirs.at[pl.ds(j * size, size), :]) for j, (at, ref) in enumerate(held)]

    def finish(found):
        for at, total, keep in found:
            parts[pl.ds(at, 1), :] = total
            kept[pl.ds(at, 1), :] = keep

    read_pieces(
        pieces, query, query_gain, shift, (score_ref, weight_ref), keys, values, sems, finish, scale
    )


def late_body(
    query, query_gain, out_gain, shift, f3, theirs, parts, kept, *rest, scale, chips
):
    keys, values, first, part_ref, kept_ref, score_ref, weight_ref, sems = rest[2:]
    _, far = positions(chips)
    pieces = [(far[3], f3, theirs)]
    part_ref[...] = parts[...]
    kept_ref[...] = kept[...]

    def finish(found):
        for at, total, keep in found:
            part_ref[pl.ds(at, 1), :] = total
            kept_ref[pl.ds(at, 1), :] = keep
        row = lax.broadcasted_iota(jnp.int32, (chips, chips), 0)
        up = (lax.broadcasted_iota(jnp.int32, (chips, chips), 1) > row).astype(jnp.float32)
        later = jnp.dot(
            up, kept_ref[...], precision=lax.Precision.HIGHEST, preferred_element_type=jnp.float32
        )
        total = jnp.exp(jnp.sum(later, axis=1, keepdims=True)) * part_ref[...]
        total = jnp.sum(total, axis=0, keepdims=True)
        first[...] = row_norm(total, out_gain[...]).astype(jnp.bfloat16)

    read_pieces(
        pieces, query, query_gain, shift, (score_ref, weight_ref), keys, values, sems, finish, scale
    )


def in_vmem(n):
    return [pl.BlockSpec(memory_space=pltpu.VMEM)] * n


def shape(*dims, dtype=jnp.bfloat16):
    return jax.ShapeDtypeStruct(dims, dtype)


def shards(
    layer_input,
    input_gain,
    key_weight,
    value_weight,
    key_gain,
    stop_shift,
    new_query,
    query_gain,
    out_gain,
):
    groups = lax.axis_size("tp")
    n_sp = lax.axis_size("sp")
    nz, ny = n_sp // NX, groups // 2
    rows, width = layer_input.shape[1:]
    size = 2 * rows
    head_size = new_query.shape[2]
    length = rows * groups
    cols = KVH * head_size
    deep = width // n_sp

    sent = pl.pallas_call(
        pack_body,
        out_shape=shape(groups, 24, 128),
        in_specs=[pl.BlockSpec(memory_space=pltpu.HBM)] * 3,
        out_specs=in_vmem(1)[0],
        scratch_shapes=[
            pltpu.VMEM(key_weight.shape[::-1], jnp.bfloat16),
            pltpu.VMEM(key_weight.shape[::-1], jnp.bfloat16),
            pltpu.VMEM(stop_shift.shape[1:], jnp.bfloat16),
            pltpu.SemaphoreType.DMA((3,)),
        ],
        compiler_params=pltpu.CompilerParams(vmem_limit_bytes=4 * MIB),
        name="pack",
    )(
        *(
            pltpu.with_memory_space_constraint(a, pltpu.HBM)
            for a in (key_weight.T, value_weight.T, stop_shift[0])
        )
    )
    recv = lax.all_to_all(sent, "tp", split_axis=0, concat_axis=0, tiled=True)
    blocks, shift48, shift_line = pl.pallas_call(
        build_body,
        out_shape=(
            shape(nz, deep, cols),
            shape(length // 128, 128, dtype=jnp.float32),
            shape(1, 1, length),
        ),
        in_specs=in_vmem(1),
        out_specs=tuple(in_vmem(3)),
        scratch_shapes=[
            pltpu.VMEM((cols, deep), jnp.bfloat16),
            pltpu.VMEM((length // 128, 128), jnp.float32),
        ],
        compiler_params=pltpu.CompilerParams(vmem_limit_bytes=8 * MIB),
        name="build",
    )(recv)

    own = pl.pallas_call(
        norm_body,
        grid=(4,),
        out_shape=shape(rows, width),
        in_specs=[
            pl.BlockSpec((rows // 4, width), lambda i: (i, 0)),
            pl.BlockSpec((1, width), lambda i: (0, 0)),
        ],
        out_specs=pl.BlockSpec((rows // 4, width), lambda i: (i, 0)),
        compiler_params=pltpu.CompilerParams(vmem_limit_bytes=16 * MIB),
        name="norm",
    )(
        pltpu.with_memory_space_constraint(layer_input[0], pltpu.HBM),
        pltpu.with_memory_space_constraint(input_gain.reshape(1, width), pltpu.HBM),
    )
    other = swapped(own)

    classes = [[z * NX + (c + 2 * z) % NX for z in range(nz)] for c in range(CLASSES)]
    got = lax.all_to_all(
        blocks, "sp", split_axis=0, concat_axis=0, tiled=True, axis_index_groups=classes
    )
    w0 = got.reshape(nz * deep, cols)
    half = nz * deep // 2
    wl = moved_sp(w0, 0, 1)
    wr = moved_sp(w0, 0, -1)
    wu = moved_sp(w0[:half], 1, 0)
    wd = moved_sp(w0[half:], -1, 0)
    acc_shape = shape(2, rows, cols, dtype=jnp.float32)
    acc = pl.pallas_call(
        first_body,
        out_shape=acc_shape,
        in_specs=in_vmem(3),
        out_specs=in_vmem(1)[0],
        cost_estimate=pl.CostEstimate(flops=4 * rows * half * cols * 2, bytes_accessed=0, transcendentals=0),
        compiler_params=pltpu.CompilerParams(vmem_limit_bytes=16 * MIB),
        name="first",
    )(own, other, w0)
    acc = pl.pallas_call(
        sides_body,
        out_shape=acc_shape,
        in_specs=in_vmem(5),
        out_specs=in_vmem(1)[0],
        input_output_aliases={4: 0},
        cost_estimate=pl.CostEstimate(flops=8 * rows * half * cols * 2, bytes_accessed=0, transcendentals=0),
        compiler_params=pltpu.CompilerParams(vmem_limit_bytes=16 * MIB),
        name="sides",
    )(own, other, wl, wr, acc)
    slots = pl.pallas_call(
        last_body,
        out_shape=tuple(shape(size, head_size) for _ in range(4)),
        in_specs=in_vmem(6),
        out_specs=tuple(in_vmem(4)),
        scratch_shapes=[pltpu.VMEM((size, cols), jnp.bfloat16)],
        cost_estimate=pl.CostEstimate(flops=4 * rows * half * cols * 2, bytes_accessed=0, transcendentals=0),
        compiler_params=pltpu.CompilerParams(vmem_limit_bytes=20 * MIB),
        name="last",
    )(own, other, wu, wd, acc, key_gain.reshape(1, head_size))

    def across(at):
        return at ^ 1

    mine = slots[0]
    p1 = moved_y(slots[1], step_to(1))
    p2 = moved_y(slots[2], step_to(2))
    p3 = moved_y(slots[3], step_to(3))
    f0 = moved_y(mine, across)
    f12 = moved_y(jnp.concatenate((p1, p2), 0), across)
    f3 = moved_y(p3, across)
    t1 = swapped(jnp.concatenate((mine, f0, p1, p2, p3, f12), 0))
    t2 = swapped(f3)
    in_hbm = pl.BlockSpec(memory_space=pltpu.HBM)
    scale = 1.0 / head_size**0.5
    line_shape = shape(length, head_size)
    part_shape = shape(ny, head_size, dtype=jnp.float32)
    query, gain_q, gain_o = new_query[0], query_gain.reshape(1, -1), out_gain.reshape(1, -1)
    per = size // 128

    def scratch(n):
        lines = [pltpu.VMEM((n * per, 128), jnp.float32)] * 2
        return [*lines, pltpu.SemaphoreType.DMA((2 * n,))]

    early = pl.pallas_call(
        lambda *refs: early_body(*refs, scale=scale, chips=ny),
        out_shape=(line_shape, line_shape, part_shape, part_shape),
        in_specs=in_vmem(10),
        out_specs=(in_hbm, in_hbm, *in_vmem(2)),
        scratch_shapes=scratch(7),
        compiler_params=pltpu.CompilerParams(vmem_limit_bytes=16 * MIB),
        name="early",
    )
    key_line, value_line, parts, kept = early(query, gain_q, shift48, mine, f0, p1, p2, p3, f12, t1)
    key_line, value_line, first_out = pl.pallas_call(
        lambda *refs: late_body(*refs, scale=scale, chips=ny),
        out_shape=(line_shape, line_shape, shape(1, head_size)),
        in_specs=in_vmem(8) + [in_hbm] * 2,
        out_specs=(in_hbm, in_hbm, in_vmem(1)[0]),
        scratch_shapes=[
            pltpu.VMEM((ny, head_size), jnp.float32),
            pltpu.VMEM((ny, head_size), jnp.float32),
            *scratch(1),
        ],
        input_output_aliases={8: 0, 9: 1},
        compiler_params=pltpu.CompilerParams(vmem_limit_bytes=16 * MIB),
        name="late",
    )(query, gain_q, gain_o, shift48, f3, t2, parts, kept, key_line, value_line)
    return (
        key_line.reshape(1, 1, length, head_size),
        value_line.reshape(1, 1, length, head_size),
        shift_line,
        first_out[None],
    )


def solution(mesh):
    placed = (
        P("sp", "tp", None),
        P(),
        P("sp", "tp"),
        P("sp", "tp"),
        P(),
        P("sp", None, "tp"),
        P("sp", "tp", None),
        P(),
        P(),
    )
    return jax.shard_map(
        shards,
        mesh=mesh,
        in_specs=placed,
        out_specs=(
            P("sp", "tp", None, None),
            P("sp", "tp", None, None),
            P("sp", "tp", None),
            P("sp", "tp", None),
        ),
        check_vma=False,
    )
```
